512 devices in a mesh: dp: 4 (over x), kv: 64 (over z, y), tp: 2 (over core).
Axes of the slice: x: 4, y: 4, z: 16, core: 2. Of those that a mesh axis runs over, the one named last changes fastest.
Arguments:
- tokens: bfloat16 [4, 20480, 2048], P('dp', 'kv'), may hold values from -72 to 72
- w_query: bfloat16 [2048, 512], P(None, 'tp'), may hold values from -0.125 to 0.125
- key_weight: bfloat16 [2048, 256], P(None, 'tp'), may hold values from -0.125 to 0.125
- value_weight: bfloat16 [2048, 256], P(None, 'tp'), may hold values from -2.09375 to 2.09375
- w_out: bfloat16 [512, 2048], P(None, 'tp'), may hold values from -0.25 to 0.25
- chosen: int32 [4, 640, 16], P('dp', 'kv'), may hold values from -1 to 639, as said below
Outputs:
- mixed: bfloat16 [4, 20480, 2048], P('dp', 'kv', 'tp')
- log_mass: float32 [4, 4, 20480], P('dp', 'tp', 'kv')
The draws below stay inside these ranges and needn't reach their ends.
Inputs may be any that keep to these rules, and one draw needn't show every extreme that they name: `chosen`: entry 0 of row i of a sequence is i; the other entries are distinct blocks before i, or -1 for an empty slot. The 10 rows of one index of kv together name at most one block held by any other index of kv; this bound is reached.
All inputs are finite; a program needn't handle non-finite values.
Results may differ from the reference program's by a relative error of at most 0.006.
The reference program's roundings to bfloat16 on the way (of `queries`, `probs_low` and `attended`) count: a program that leaves them out, or rounds other values in their place, can miss the bound.
Values may be sent and summed in bfloat16 or wider, within the bound.
A program may use at most 64 MiB of HBM per device.

```python
import jax
import jax.numpy as jnp
from jax import lax

MODEL_WIDTH = 2048
HEAD_WIDTH = 128
QUERY_HEAD_COUNT = 4
KEY_VALUE_HEADS = 2
BLOCK_POSITIONS = 32
CHOSEN_SLOTS = 16
BLK_DEV = 10
SEQUENCE_BLOCKS = 640
SEQ = 20480
SEQS = 4
N_KV = 64


def draw_tokens(key, part):
    base = jnp.clip(jax.random.normal(jax.random.fold_in(key, 21), (SEQS, SEQ, MODEL_WIDTH), jnp.float32), -6.0, 6.0)
    return base.astype(jnp.bfloat16)


def draw_chosen(key, part):
    popular = (jax.random.randint(jax.random.fold_in(key, 11), (SEQS, 1, N_KV), 0, 6) == 0).astype(jnp.int32)
    noise = jax.random.randint(jax.random.fold_in(key, 12), (SEQS, N_KV, N_KV), 0, 65536)
    block_pick = jax.random.randint(jax.random.fold_in(key, 13), (SEQS, N_KV, N_KV), 0, BLK_DEV)
    device_ix = jnp.arange(N_KV, dtype=jnp.int32)[:, None]
    owner_ix = jnp.arange(N_KV, dtype=jnp.int32)[None, :]
    forced = ((owner_ix == device_ix - 1) | (owner_ix == device_ix - N_KV // 2)).astype(jnp.int32)
    ranks = (forced * 3 + popular) * 65536 + noise
    ranks = jnp.where(owner_ix < device_ix, ranks, -1)
    ranking = jnp.argsort(-ranks, axis=-1, stable=True).astype(jnp.int32)
    spare = CHOSEN_SLOTS - BLK_DEV
    rows_out = []
    for inner_ix in range(BLK_DEV):
        slot_ix = inner_ix * spare + jnp.arange(spare, dtype=jnp.int32)
        live_slot = slot_ix[None, :] < device_ix
        bounded_index = jnp.minimum(slot_ix, N_KV - 1)
        chosen_owner = jnp.take(ranking, bounded_index, axis=2)
        chosen_block = chosen_owner * BLK_DEV + jnp.take_along_axis(block_pick, chosen_owner, axis=2)
        far_part = jnp.where(live_slot[None], chosen_block, -1)
        own_block = jnp.broadcast_to((device_ix * BLK_DEV + inner_ix)[None], (SEQS, N_KV, 1))
        near_cols = []
        for earlier in range(BLK_DEV - 1):
            column = jnp.where(earlier < inner_ix, device_ix * BLK_DEV + earlier, -1)
            near_cols.append(jnp.broadcast_to(column[None], (SEQS, N_KV, 1)))
        rows_out.append(jnp.concatenate([own_block] + near_cols + [far_part], axis=2))
    return jnp.stack(rows_out, axis=2).reshape(SEQS, SEQUENCE_BLOCKS, CHOSEN_SLOTS).astype(jnp.int32)


def shard_levels(rng, extent, cuts, low, high):
    def one(axis_at, shards_of):
        steps = jax.random.uniform(jax.random.fold_in(jax.random.fold_in(rng, 6), axis_at), (shards_of,), jnp.float32, low / len(cuts), high / len(cuts))
        return jnp.repeat(jnp.exp(steps), extent[axis_at] // shards_of).reshape((-1,) + (1,) * (len(extent) - axis_at - 1))

    level = one(*cuts[0])
    for cut in cuts[1:]:
        level = level * one(*cut)
    return level


def centred(rng, extent, scale, most, pieces=(), kind=jnp.bfloat16):
    drawn = scale * jax.random.normal(rng, extent, jnp.float32)
    if pieces:
        drawn = drawn * shard_levels(rng, extent, pieces, -0.22, 0.18)
    return jnp.clip(drawn, -most, most).astype(kind)


def setup_inputs(seed: int = 0) -> dict:
    arg_keys = jax.random.split(jax.random.key(seed), 7)
    return {
        "tokens": draw_tokens(jax.random.fold_in(arg_keys[6], 71), 0),
        "w_query": centred(arg_keys[1], (MODEL_WIDTH, QUERY_HEAD_COUNT * HEAD_WIDTH), MODEL_WIDTH ** -0.5, 0.125, ((1, 2),)),
        "key_weight": centred(arg_keys[2], (MODEL_WIDTH, KEY_VALUE_HEADS * HEAD_WIDTH), MODEL_WIDTH ** -0.5, 0.125, ((1, 2),)),
        "value_weight": centred(arg_keys[3], (MODEL_WIDTH, KEY_VALUE_HEADS * HEAD_WIDTH), 0.35, 2.09375, ((1, 2),)),
        "w_out": centred(arg_keys[4], (QUERY_HEAD_COUNT * HEAD_WIDTH, MODEL_WIDTH), (QUERY_HEAD_COUNT * HEAD_WIDTH) ** -0.5, 0.25, ((1, 2),)),
        "chosen": draw_chosen(jax.random.fold_in(arg_keys[6], 71), 0),
    }


def attend_block(entry, key_block_table, value_block_table):
    query_block_rows, row_chosen, block_index = entry
    heads_per_group = QUERY_HEAD_COUNT // KEY_VALUE_HEADS
    bounded_index = jnp.maximum(row_chosen, 0)
    selected_keys = key_block_table[bounded_index].reshape(CHOSEN_SLOTS * BLOCK_POSITIONS, KEY_VALUE_HEADS, HEAD_WIDTH)
    selected_values = value_block_table[bounded_index].reshape(CHOSEN_SLOTS * BLOCK_POSITIONS, KEY_VALUE_HEADS, HEAD_WIDTH)
    grouped_queries = query_block_rows.reshape(BLOCK_POSITIONS, KEY_VALUE_HEADS, heads_per_group, HEAD_WIDTH)
    scores = jnp.einsum('tkgd,skd->kgts', grouped_queries.astype(jnp.float32), selected_keys.astype(jnp.float32)) * (HEAD_WIDTH ** -0.5)
    key_pos = (bounded_index[:, None] * BLOCK_POSITIONS + jnp.arange(BLOCK_POSITIONS, dtype=jnp.int32)[None, :]).reshape(CHOSEN_SLOTS * BLOCK_POSITIONS)
    key_live = jnp.repeat(row_chosen >= 0, BLOCK_POSITIONS)
    query_pos = block_index * BLOCK_POSITIONS + jnp.arange(BLOCK_POSITIONS, dtype=jnp.int32)
    allowed = key_live[None, :] & (key_pos[None, :] <= query_pos[:, None])
    scores = jnp.where(allowed, scores, -jnp.inf)
    row_max = jnp.max(scores, axis=-1)
    weights = jnp.exp(scores - row_max[..., None])
    row_sum = jnp.sum(weights, axis=-1)
    probs_low = lax.optimization_barrier(weights.astype(jnp.bfloat16))
    summed = jnp.einsum('kgts,skd->tkgd', probs_low.astype(jnp.float32), selected_values.astype(jnp.float32))
    attended = (summed / row_sum.transpose(2, 0, 1)[..., None]).astype(jnp.bfloat16).reshape(BLOCK_POSITIONS, QUERY_HEAD_COUNT * HEAD_WIDTH)
    log_part = (row_max + jnp.log(row_sum)).reshape(QUERY_HEAD_COUNT, BLOCK_POSITIONS)
    return attended, log_part


def reference(tokens, w_query, key_weight, value_weight, w_out, chosen):
    def one_sequence(entry):
        seq_tokens, seq_chosen = entry
        queries = jnp.dot(seq_tokens, w_query, preferred_element_type=jnp.float32).astype(jnp.bfloat16)
        projected_keys = jnp.dot(seq_tokens, key_weight, preferred_element_type=jnp.float32).astype(jnp.bfloat16)
        projected_values = jnp.dot(seq_tokens, value_weight, preferred_element_type=jnp.float32).astype(jnp.bfloat16)
        queries = queries.reshape(SEQUENCE_BLOCKS, BLOCK_POSITIONS, QUERY_HEAD_COUNT, HEAD_WIDTH)
        key_block_table = projected_keys.reshape(SEQUENCE_BLOCKS, BLOCK_POSITIONS, KEY_VALUE_HEADS, HEAD_WIDTH)
        value_block_table = projected_values.reshape(SEQUENCE_BLOCKS, BLOCK_POSITIONS, KEY_VALUE_HEADS, HEAD_WIDTH)

        def per_block(item_entry):
            return attend_block(item_entry, key_block_table, value_block_table)

        attended, log_part = lax.map(per_block, (queries, seq_chosen, jnp.arange(SEQUENCE_BLOCKS, dtype=jnp.int32)))
        attended = attended.reshape(SEQ, QUERY_HEAD_COUNT * HEAD_WIDTH)
        mixed = jnp.dot(attended, w_out, preferred_element_type=jnp.float32).astype(jnp.bfloat16)
        return mixed, log_part.transpose(1, 0, 2).reshape(QUERY_HEAD_COUNT, SEQ)

    mixed_all, log_all = lax.map(one_sequence, (tokens, chosen))
    return mixed_all, log_all
```

```python
import functools

import jax
import jax.numpy as jnp
from jax import lax
from jax.experimental import pallas as pl
from jax.experimental.pallas import tpu as pltpu
from jax.sharding import PartitionSpec as P

HEAD_WIDTH = 128
RING_Y = 4
BLOCKS_PER_CHUNK = 2
MASKED = -1e38
LOG2_E = 1.4426950408889634
LN_2 = 0.6931471805599453
SCORE_SCALE = HEAD_WIDTH ** (-0.5) * LOG2_E
MESH = pl.DeviceIdType.MESH
COLUMN_TILE = 128
DEPTH_PARTS = 2
MIX_PARTS = 4
LAG = (9, 2)


def exchange_kernel(
    ring_z,
    blocks_here,
    block_rows,
    tokens_hbm,
    wq_hbm,
    wk_hbm,
    wv_hbm,
    wo_hbm,
    chosen_hbm,
    partner,
    log_out,
    wo,
    own_mixed,
    tok,
    wkv,
    wq,
    kv_sum,
    chosen,
    kvbuf,
    stage,
    table,
    outbox,
    qx,
    m_ref,
    l_ref,
    acc,
    keys_in,
    values_in,
    by_row,
    attended,
    want_all,
    want_smem,
    load_sem,
    part_sem,
    plus_send,
    plus_recv,
    minus_send,
    minus_recv,
    y_send,
    y_recv,
    want_send,
    want_recv,
    tp_send,
    tp_recv,
):
    f32, bf16 = jnp.float32, jnp.bfloat16
    me = lax.axis_index("kv")
    core = lax.axis_index("tp")
    z, y = me // RING_Y, me % RING_Y
    rows = blocks_here * block_rows
    half = ring_z // 2
    wrap_last = half - 2
    chunks = blocks_here // BLOCKS_PER_CHUNK
    up = ((z + 1) % ring_z) * RING_Y + y
    down = ((z + ring_z - 1) % ring_z) * RING_Y + y

    side = [z * RING_Y + (y + d) % RING_Y for d in range(RING_Y)]
    beyond = {
        dz: [((z + dz) % ring_z) * RING_Y + (y + d) % RING_Y for d in range(RING_Y)]
        for dz in (1, ring_z - 1)
    }
    barrier = pltpu.get_barrier_semaphore()
    for peer in [up, down] + side[1:]:
        pl.semaphore_signal(barrier, inc=1, device_id={"kv": peer}, device_id_type=MESH)
    pl.semaphore_signal(barrier, inc=1, device_id={"tp": 1 - core}, device_id_type=MESH)

    part_depth = tok.shape[1] // DEPTH_PARTS

    def loads_of(i):
        deep = pl.ds(pl.multiple_of(i * part_depth, part_depth), part_depth)
        k_lanes, v_lanes = pl.ds(0, HEAD_WIDTH), pl.ds(HEAD_WIDTH, HEAD_WIDTH)
        return [
            pltpu.make_async_copy(tokens_hbm.at[0, :, deep], tok.at[:, deep], part_sem.at[i, 0]),
            pltpu.make_async_copy(wk_hbm.at[deep], wkv.at[deep, k_lanes], part_sem.at[i, 1]),
            pltpu.make_async_copy(wv_hbm.at[deep], wkv.at[deep, v_lanes], part_sem.at[i, 2]),
        ]

    load_chosen = pltpu.make_async_copy(chosen_hbm, chosen, load_sem.at[0])
    load_wq = pltpu.make_async_copy(wq_hbm, wq, load_sem.at[1])
    load_wo = pltpu.make_async_copy(wo_hbm, wo, load_sem.at[2])
    load_chosen.start()
    for i in range(DEPTH_PARTS):
        for load in loads_of(i):
            load.start()

    with jax.named_scope("project_kv"):
        kv_sum[...] = jnp.zeros_like(kv_sum)

        @pl.loop(0, DEPTH_PARTS)
        def _(i):
            for load in loads_of(i):
                load.wait()
            deep = pl.ds(pl.multiple_of(i * part_depth, part_depth), part_depth)
            kv_sum[...] += jnp.dot(tok[:, deep], wkv[deep, :], preferred_element_type=f32)

        load_wq.start()
        load_wo.start()
        own = kv_sum[...].astype(bf16)
        for i in range(blocks_here):
            kvbuf[0, i] = own[i * block_rows : (i + 1) * block_rows, :]

    with jax.named_scope("barrier"):
        pl.semaphore_wait(barrier, RING_Y + 2)

    def ring_copy(going_up, src_slot, dst_slot, c):
        view = pl.ds(c * BLOCKS_PER_CHUNK, BLOCKS_PER_CHUNK)
        step = dst_slot if going_up else ring_z - dst_slot
        return pltpu.make_async_remote_copy(
            src_ref=kvbuf.at[src_slot, view],
            dst_ref=kvbuf.at[dst_slot, view],
            send_sem=(plus_send if going_up else minus_send).at[0],
            recv_sem=(plus_recv if going_up else minus_recv).at[step - 1, c],
            device_id={"kv": up if going_up else down},
            device_id_type=MESH,
        )

    def sent(ref, sem, count):
        view = ref.at[pl.ds(0, count)]
        pltpu.make_async_remote_copy(
            src_ref=view,
            dst_ref=view,
            send_sem=sem,
            recv_sem=plus_recv.at[0, 0],
            device_id={"kv": up},
            device_id_type=MESH,
        ).wait_send()

    last_up, last_down = half - 2, half - 1

    def from_below(t):
        return (z >= t) & (t <= last_up)

    def to_above(t):
        return (z >= t) & (z < ring_z - 1) & (t < last_up)

    def from_above(t):
        return ((z + t) % ring_z <= last_down) & (t <= last_down)

    def to_below(t):
        source = (z + t) % ring_z
        return (source <= last_down) & (t < last_down)

    chosen_up = (z >= last_up) & (z < ring_z - 1)
    chosen_down = (z + last_down) % ring_z <= last_down

    with jax.named_scope("first_sends"):
        for c in range(chunks):

            @pl.when(to_above(0))
            def _():
                ring_copy(True, 0, 1, c).start()

            @pl.when(to_below(0))
            def _():
                ring_copy(False, 0, ring_z - 1, c).start()

    lanes = RING_Y * ring_z
    load_chosen.wait()
    lane = lax.broadcasted_iota(jnp.int32, (blocks_here, 128), 1)
    back_y, back_z = lane // ring_z, lane % ring_z
    source = ((z - back_z + ring_z) % ring_z) * RING_Y + (y - back_y + RING_Y) % RING_Y
    low = jnp.where(lane < lanes, source * blocks_here, me * blocks_here + lane - lanes)
    width = jnp.where(
        lane == 0,
        0,
        jnp.where(lane < lanes, blocks_here, jnp.where(lane < lanes + blocks_here, 1, 0)),
    )
    best = jnp.full((blocks_here, 128), -1, jnp.int32)
    picks = chosen[...].reshape(blocks_here, chosen.shape[2])
    for slot in range(chosen.shape[2]):
        inner = picks[:, slot : slot + 1] - low
        best = jnp.where((inner >= 0) & (inner < width), inner, best)
    mask_rows = jnp.where(best >= 0, 0.0, MASKED).astype(f32)
    want = jnp.maximum(best[0:1, :], 0)
    for i in range(1, blocks_here):
        want = jnp.maximum(want, best[i : i + 1, :])
    want_all[0] = want
    def want_copy(source, target, sem, peer):
        return pltpu.make_async_remote_copy(
            src_ref=want_all.at[source],
            dst_ref=want_all.at[target],
            send_sem=want_send.at[sem],
            recv_sem=want_recv.at[sem],
            device_id={"kv": peer},
            device_id_type=MESH,
        )

    row = pl.ds(0, RING_Y)
    rest = pl.ds(1, RING_Y - 1)
    want_side = want_copy(rest, rest, 0, up)
    want_up = want_copy(row, pl.ds(2 * RING_Y, RING_Y), 1, up)
    want_down = want_copy(row, pl.ds(RING_Y, RING_Y), 2, down)
    for d in (2, 1, 3):
        want_copy(0, RING_Y - d, 0, side[d]).start()

    for head in range(qx.shape[0] // rows):
        for i in range(blocks_here):
            qx[pl.ds(head * rows + i * block_rows, block_rows), HEAD_WIDTH:] = jnp.broadcast_to(
                mask_rows[i : i + 1, :], (block_rows, 128)
            ).astype(bf16)

    for slot in range(1, ring_z):

        @pl.when(z < slot)
        def _():
            table[slot] = jnp.zeros(table.shape[1:], bf16)

    with jax.named_scope("project_q"):
        load_wq.wait()
        queries = jnp.dot(tok[...], wq[...], preferred_element_type=f32).astype(bf16)
        heads = qx.shape[0] // rows
        for head in range(heads):
            qx[pl.ds(head * rows, rows), 0:HEAD_WIDTH] = queries[
                :, head * HEAD_WIDTH : (head + 1) * HEAD_WIDTH
            ]

    columns = qx.shape[0]
    tiles = columns // COLUMN_TILE

    def attend(tile, count, first):
        begin, size = (0, columns) if tile is None else (tile * COLUMN_TILE, COLUMN_TILE)
        here = pl.ds(begin, size)
        s = lax.dot_general(
            keys_in[0:count, :],
            qx[here, :],
            (((1,), (1,)), ((), ())),
            preferred_element_type=f32,
        ) * SCORE_SCALE
        if first:
            row = lax.broadcasted_iota(jnp.int32, s.shape, 1) + begin
            row = jnp.where(row >= rows, row - rows, row)
            s = jnp.where(lax.broadcasted_iota(jnp.int32, s.shape, 0) <= row, s, MASKED)
        top = jnp.max(s, axis=0, keepdims=True)
        if first:
            new_m = top
        else:
            old_m = m_ref[:, here]
            new_m = jnp.maximum(old_m, top)
            shrink = jnp.exp2(old_m - new_m)
        p = jnp.exp2(s - new_m)
        total = jnp.sum(p, axis=0, keepdims=True)
        summed = jnp.dot(values_in[:, 0:count], p.astype(bf16), preferred_element_type=f32)
        m_ref[:, here] = new_m
        if first:
            l_ref[:, here] = total
            acc[:, here] = summed
        else:
            l_ref[:, here] = l_ref[:, here] * shrink + total
            acc[:, here] = acc[:, here] * shrink + summed

    def attend_own():
        key_lane = lax.broadcasted_iota(jnp.int32, (rows, 128), 1)
        key_block = lax.broadcasted_iota(jnp.int32, (rows, 128), 0) // block_rows
        own_hot = jnp.where(key_lane == key_block + lanes, 1.0, 0.0).astype(bf16)
        own = kvbuf[0].reshape(rows, 2 * HEAD_WIDTH)
        keys_in[0:rows, 0:HEAD_WIDTH] = own[:, 0:HEAD_WIDTH]
        keys_in[0:rows, HEAD_WIDTH:] = own_hot
        values_in[:, 0:rows] = own[:, HEAD_WIDTH:].T
        attend(None, rows, True)

    def arrival(slot):
        return y_recv.at[jnp.where(slot > half + 1, ring_z - slot, slot)]

    def chosen_copy(d, slot, peer, kind):
        return pltpu.make_async_remote_copy(
            src_ref=outbox.at[slot, d],
            dst_ref=table.at[slot, d],
            send_sem=y_send.at[kind],
            recv_sem=arrival(slot),
            device_id={"kv": peer},
            device_id_type=MESH,
        )

    def arrived(slot, count, first):
        view = table.at[pl.ds(0, count), pl.ds(first, RING_Y - first)]
        pltpu.make_async_remote_copy(
            src_ref=view,
            dst_ref=view,
            send_sem=y_send.at[0],
            recv_sem=arrival(slot),
            device_id={"kv": up},
            device_id_type=MESH,
        ).wait_recv()

    def pass_on(slot):
        stage[...] = kvbuf[slot]
        for d in (2, 1, 3):
            outbox[slot, d] = stage[want_smem[d, 0, d * ring_z + slot]]
            chosen_copy(d, slot, side[d], 0).start()
        table[slot, 0] = stage[want_smem[0, 0, slot]]

    def pass_beyond(dz, held, slot):
        stage[...] = kvbuf[held]
        for d in (2, 1, 3, 0):
            row_there = (RING_Y if dz == 1 else 2 * RING_Y) + d
            outbox[slot, d] = stage[want_smem[row_there, 0, d * ring_z + slot]]
            chosen_copy(d, slot, beyond[dz][d], 1 if dz == 1 else 2).start()

    near_keys = RING_Y * block_rows

    def attend_slots(tile, slots):
        if not tile:
            lane_row = lax.broadcasted_iota(jnp.int32, (near_keys, 128), 1)
            back = lax.broadcasted_iota(jnp.int32, (near_keys, 128), 0) // block_rows * ring_z
            for i, slot in enumerate(slots):
                both = table[slot].reshape(near_keys, 2 * HEAD_WIDTH)
                here = slice(i * near_keys, (i + 1) * near_keys)
                keys_in[here, 0:HEAD_WIDTH] = both[:, 0:HEAD_WIDTH]
                keys_in[here, HEAD_WIDTH:] = jnp.where(
                    lane_row == back + slot, 1.0, 0.0
                ).astype(bf16)
                values_in[:, here] = both[:, HEAD_WIDTH:].T
        attend(tile, len(slots) * near_keys, False)

    def due_from_above(t, c):
        behind = (t - 1) * chunks + c - (LAG[0] * (ring_z - 1 - z)) // LAG[1]
        m = jnp.maximum(behind, 0)
        crossed = z > last_down
        hops = jnp.where(crossed, m // chunks + ring_z - z, t)
        chunk = jnp.where(crossed, m % chunks, c)
        due = jnp.where(crossed, (behind >= 0) & (hops <= last_down), from_above(t))
        return due, hops, chunk

    def step(t, fill):
        for c in range(chunks):

            @pl.when(from_below(t))
            def _():
                ring_copy(True, t, t, c).wait_recv()

            @pl.when(to_above(t))
            def _():
                ring_copy(True, t, t + 1, c).start()

            due, hops, chunk = due_from_above(t, c)
            back = ring_z - hops

            @pl.when(due)
            def _():
                ring_copy(False, back, back, chunk).wait_recv()

            @pl.when(due & (hops < last_down))
            def _():
                ring_copy(False, back, back - 1, chunk).start()

            @pl.when(due & (chunk == chunks - 1) & (hops == last_down) & chosen_down)
            def _():
                pass_beyond(ring_z - 1, ring_z - last_down, half)

            @pl.when(due & (chunk == chunks - 1) & (z >= back))
            def _():
                pass_on(back)

            if c < chunks - 1:
                fill(c)

        if t is last_up:

            @pl.when(chosen_up)
            def _():
                pass_beyond(1, last_up, last_up + 1)

        if t is not last_down:

            @pl.when(z >= t)
            def _():
                pass_on(t)

        fill(chunks - 1)

    def near_slots(t):
        @pl.when((z >= t) & (z < ring_z - t))
        def _():
            arrived(t, 1, 1)

        @pl.when(z >= ring_z - t)
        def _():
            arrived(t, 2, 1)

    near_scalars = pltpu.make_async_copy(want_all.at[row], want_smem.at[row], load_sem.at[3])
    far_rows = pl.ds(RING_Y, 2 * RING_Y)
    far_scalars = pltpu.make_async_copy(want_all.at[far_rows], want_smem.at[far_rows], load_sem.at[3])

    def fill_first(c):
        if c == 1:
            want_side.wait()
            want_up.start()
            want_down.start()
            near_scalars.start()
        if c == chunks - 2:
            near_scalars.wait()
            pass_on(0)

    def fill_second(c):
        if c == chunks - 1:
            want_up.wait()
            want_down.wait()
            far_scalars.start()
            arrived(0, 1, 1)
            attend_slots(None, [0])
            far_scalars.wait()

    def fill_near(t, c):
        if c == 1:
            near_slots(t)
        for tile in {0: [], 1: [0], 2: [1, 2], 3: [3], 4: [4]}[c]:

            @pl.when(z >= t)
            def _():
                attend_slots(tile, [t, ring_z - t])

    share = pltpu.make_async_remote_copy(
        src_ref=attended,
        dst_ref=partner,
        send_sem=tp_send,
        recv_sem=tp_recv,
        device_id={"tp": 1 - core},
        device_id_type=MESH,
    )

    def finish():
        with jax.named_scope("normalise"):
            for tile in range(tiles):
                here = slice(tile * COLUMN_TILE, (tile + 1) * COLUMN_TILE)
                by_row[here, :] = (acc[:, here] / l_ref[:, here]).T.astype(bf16)
            for h in range(heads):
                attended[:, h * HEAD_WIDTH : (h + 1) * HEAD_WIDTH] = by_row[
                    h * rows : (h + 1) * rows, :
                ]
            share.start()
            load_wo.wait()
            width = heads * HEAD_WIDTH
            mine = pl.ds(pl.multiple_of(core * width, width), width)
            own_mixed[...] = jnp.dot(attended[...], wo[mine, :], preferred_element_type=f32)

        mass = m_ref[...] * LN_2 + jnp.log(l_ref[...])
        for h in range(heads):
            log_out[0, h : h + 1, :] = mass[:, h * rows : (h + 1) * rows]

    with jax.named_scope("own"):
        attend_own()
    with jax.named_scope("step_1"):
        step(1, fill_first)
    with jax.named_scope("step_2"):
        step(2, fill_second)

    @pl.loop(3, last_up)
    def _(t):
        with jax.named_scope("step_t"):
            step(t, functools.partial(fill_near, t - 2))

    @pl.when(z == 0)
    def _():
        finish()

    with jax.named_scope("step_6"):
        step(last_up, functools.partial(fill_near, last_up - 2))
    with jax.named_scope("step_7"):
        step(last_down, functools.partial(fill_near, last_down - 2))

    with jax.named_scope("last_but_one"):
        near_slots(last_up)

        @pl.when(z > last_up)
        def _():
            arrived(last_up + 1, 1, 0)

        @pl.when(z >= last_up)
        def _():
            attend_slots(None, [last_up, ring_z - last_up, last_up + 1])

    with jax.named_scope("last_wait"):

        @pl.when(z >= half)
        def _():
            arrived(half, 1, 0)

        @pl.when(z > half)
        def _():
            arrived(half + 1, 1, 1)

    with jax.named_scope("last"):

        @pl.when(z >= half)
        def _():
            attend_slots(None, [half, half + 1])

    @pl.when(z > 0)
    def _():
        finish()

    with jax.named_scope("sends"):
        ups = jnp.where(z < ring_z - 1, jnp.minimum(z + 1, last_up), 0)
        for n in range(1, last_up + 1):

            @pl.when(ups == n)
            def _():
                sent(kvbuf, plus_send.at[0], n)

        downs = jnp.where(
            z <= last_down,
            jnp.minimum(last_down + 1 - z, last_down),
            jnp.maximum(z - (ring_z - last_down), 0),
        )
        for n in range(1, last_down + 1):

            @pl.when(downs == n)
            def _():
                sent(kvbuf, minus_send.at[0], n)

        passes = jnp.minimum(z, last_up) + jnp.maximum(z - (ring_z - last_down - 1), 0) + 1
        for n in range(1, last_up + last_down + 2):

            @pl.when(passes == n)
            def _():
                sent(outbox.at[:, pl.ds(1, RING_Y - 1)], y_send.at[0], n)

        @pl.when(chosen_up)
        def _():
            sent(outbox, y_send.at[1], 1)

        @pl.when(chosen_down)
        def _():
            sent(outbox, y_send.at[2], 1)

    share.wait()


def mix_kernel(partner, wo, own_mixed, log_in, mixed_hbm, log_hbm, mixed, log_vmem, sem):
    width = partner.shape[1]
    other = 1 - lax.axis_index("tp")
    theirs = pl.ds(pl.multiple_of(other * width, width), width)
    log_vmem[...] = log_in[...]
    copies = [pltpu.make_async_copy(log_vmem, log_hbm, sem.at[0])]
    copies[0].start()
    step = wo.shape[1] // MIX_PARTS
    for i in range(MIX_PARTS):
        here = slice(i * step, (i + 1) * step)
        mixed[0, :, here] = (
            own_mixed[:, here]
            + jnp.dot(partner[...], wo[theirs, here], preferred_element_type=jnp.float32)
        ).astype(jnp.bfloat16)
        copy = pltpu.make_async_copy(
            mixed.at[:, :, pl.ds(i * step, step)], mixed_hbm.at[:, :, pl.ds(i * step, step)], sem.at[i + 1]
        )
        copy.start()
        copies.append(copy)
    for copy in copies:
        copy.wait()


def body(tokens, w_query, key_weight, value_weight, w_out, chosen):
    row_count, depth = tokens.shape[1], tokens.shape[2]
    blocks_here, slots = chosen.shape[1:]
    block_rows = row_count // blocks_here
    ring_z = lax.axis_size("kv") // RING_Y
    q_width = w_query.shape[1]
    heads = q_width // HEAD_WIDTH
    kv_width = key_weight.shape[1] + value_weight.shape[1]
    chunks = blocks_here // BLOCKS_PER_CHUNK
    dma = pltpu.SemaphoreType.DMA
    vmem = pltpu.VMEM
    hbm = lambda x: pltpu.with_memory_space_constraint(x, pltpu.HBM)
    partner, log_part, wo, own_mixed = pl.pallas_call(
        functools.partial(exchange_kernel, ring_z, blocks_here, block_rows),
        out_shape=(
            vmem((row_count, q_width), jnp.bfloat16),
            vmem((1, heads, row_count), jnp.float32),
            vmem(w_out.shape, jnp.bfloat16),
            vmem((row_count, w_out.shape[1]), jnp.float32),
        ),
        in_specs=[pl.BlockSpec(memory_space=pl.ANY)] * 6,
        out_specs=(pl.BlockSpec(memory_space=vmem),) * 4,
        scratch_shapes=[
            vmem((row_count, depth), jnp.bfloat16),
            vmem((depth, kv_width), jnp.bfloat16),
            vmem((depth, q_width), jnp.bfloat16),
            vmem((row_count, kv_width), jnp.float32),
            vmem((blocks_here, 1, slots), jnp.int32),
            vmem((ring_z, blocks_here, block_rows, kv_width), jnp.bfloat16),
            vmem((blocks_here, block_rows, kv_width), jnp.bfloat16),
            vmem((ring_z, RING_Y, block_rows, kv_width), jnp.bfloat16),
            vmem((ring_z, RING_Y, block_rows, kv_width), jnp.bfloat16),
            vmem((heads * row_count, 2 * HEAD_WIDTH), jnp.bfloat16),
            vmem((1, heads * row_count), jnp.float32),
            vmem((1, heads * row_count), jnp.float32),
            vmem((HEAD_WIDTH, heads * row_count), jnp.float32),
            vmem((max(row_count, 3 * RING_Y * block_rows), 2 * HEAD_WIDTH), jnp.bfloat16),
            vmem((HEAD_WIDTH, max(row_count, 3 * RING_Y * block_rows)), jnp.bfloat16),
            vmem((heads * row_count, HEAD_WIDTH), jnp.bfloat16),
            vmem((row_count, q_width), jnp.bfloat16),
            vmem((3 * RING_Y, 1, 128), jnp.int32),
            pltpu.SMEM((3 * RING_Y, 1, 128), jnp.int32),
            dma((4,)),
            dma((DEPTH_PARTS, 3)),
            dma((1,)),
            dma((ring_z // 2 - 2, chunks)),
            dma((1,)),
            dma((ring_z // 2 - 1, chunks)),
            dma((3,)),
            dma((ring_z // 2 + 2,)),
            dma((3,)),
            dma((3,)),
            dma,
            dma,
        ],
        compiler_params=pltpu.CompilerParams(
            collective_id=0, has_side_effects=True, vmem_limit_bytes=40 * 1024 * 1024
        ),
    )(*map(hbm, (tokens, w_query, key_weight, value_weight, w_out, chosen.reshape(blocks_here, 1, slots))))
    return pl.pallas_call(
        mix_kernel,
        out_shape=(
            jax.ShapeDtypeStruct((1, row_count, w_out.shape[1]), jnp.bfloat16),
            jax.ShapeDtypeStruct((1, heads, row_count), jnp.float32),
        ),
        in_specs=[pl.BlockSpec(memory_space=vmem)] * 4,
        out_specs=(pl.BlockSpec(memory_space=pl.ANY),) * 2,
        scratch_shapes=[
            vmem((1, row_count, w_out.shape[1]), jnp.bfloat16),
            vmem((1, heads, row_count), jnp.float32),
            dma((MIX_PARTS + 1,)),
        ],
        compiler_params=pltpu.CompilerParams(vmem_limit_bytes=12 * 1024 * 1024),
    )(partner, wo, own_mixed, log_part)


def solution(mesh):
    in_specs = (
        P("dp", "kv", None),
        P(None, "tp"),
        P(None, "tp"),
        P(None, "tp"),
        P(None, "tp"),
        P("dp", "kv", None),
    )
    out_specs = (P("dp", "kv", "tp"), P("dp", "tp", "kv"))
    return jax.shard_map(body, mesh=mesh, in_specs=in_specs, out_specs=out_specs, check_vma=False)
```

```python
import functools

import jax
import jax.numpy as jnp
from jax import lax
from jax.experimental import pallas as pl
from jax.experimental.pallas import tpu as pltpu
from jax.sharding import PartitionSpec as P

HEAD_WIDTH = 128
RING_Y = 4
BLOCKS_PER_CHUNK = 2
MASKED = -1e38
LOG2_E = 1.4426950408889634
LN_2 = 0.6931471805599453
SCORE_SCALE = HEAD_WIDTH ** (-0.5) * LOG2_E
MESH = pl.DeviceIdType.MESH
COLUMN_TILE = 128
DEPTH_PARTS = 2
MIX_PARTS = 4
LAG = (9, 2)


def exchange_kernel(
    ring_z,
    blocks_here,
    block_rows,
    tokens_hbm,
    wq_hbm,
    wk_hbm,
    wv_hbm,
    wo_hbm,
    chosen_hbm,
    partner,
    log_out,
    wo,
    own_mixed,
    tok,
    wkv,
    wq,
    kv_sum,
    chosen,
    kvbuf,
    stage,
    table,
    outbox,
    qx,
    m_ref,
    l_ref,
    acc,
    keys_in,
    values_in,
    by_row,
    attended,
    want_all,
    want_smem,
    load_sem,
    part_sem,
    plus_send,
    plus_recv,
    minus_send,
    minus_recv,
    y_send,
    y_recv,
    want_send,
    want_recv,
    tp_send,
    tp_recv,
):
    f32, bf16 = jnp.float32, jnp.bfloat16
    me = lax.axis_index("kv")
    core = lax.axis_index("tp")
    z, y = me // RING_Y, me % RING_Y
    rows = blocks_here * block_rows
    half = ring_z // 2
    wrap_last = half - 2
    chunks = blocks_here // BLOCKS_PER_CHUNK
    up = ((z + 1) % ring_z) * RING_Y + y
    down = ((z + ring_z - 1) % ring_z) * RING_Y + y

    side = [z * RING_Y + (y + d) % RING_Y for d in range(RING_Y)]
    beyond = {
        dz: [((z + dz) % ring_z) * RING_Y + (y + d) % RING_Y for d in range(RING_Y)]
        for dz in (1, ring_z - 1)
    }
    barrier = pltpu.get_barrier_semaphore()
    part_depth = tok.shape[1] // DEPTH_PARTS

    def loads_of(i):
        deep = pl.ds(pl.multiple_of(i * part_depth, part_depth), part_depth)
        k_lanes, v_lanes = pl.ds(0, HEAD_WIDTH), pl.ds(HEAD_WIDTH, HEAD_WIDTH)
        return [
            pltpu.make_async_copy(tokens_hbm.at[0, :, deep], tok.at[:, deep], part_sem.at[i, 0]),
            pltpu.make_async_copy(wk_hbm.at[deep], wkv.at[deep, k_lanes], part_sem.at[i, 1]),
            pltpu.make_async_copy(wv_hbm.at[deep], wkv.at[deep, v_lanes], part_sem.at[i, 2]),
        ]

    load_chosen = pltpu.make_async_copy(chosen_hbm, chosen, load_sem.at[0])
    load_wq = pltpu.make_async_copy(wq_hbm, wq, load_sem.at[1])
    load_wo = pltpu.make_async_copy(wo_hbm, wo, load_sem.at[2])
    for i in range(DEPTH_PARTS):
        for load in loads_of(i):
            load.start()
    load_chosen.start()
    for peer in [up, down] + side[1:]:
        pl.semaphore_signal(barrier, inc=1, device_id={"kv": peer}, device_id_type=MESH)
    pl.semaphore_signal(barrier, inc=1, device_id={"tp": 1 - core}, device_id_type=MESH)


    with jax.named_scope("project_kv"):
        kv_sum[...] = jnp.zeros_like(kv_sum)

        @pl.loop(0, DEPTH_PARTS)
        def _(i):
            for load in loads_of(i):
                load.wait()
            deep = pl.ds(pl.multiple_of(i * part_depth, part_depth), part_depth)
            kv_sum[...] += jnp.dot(tok[:, deep], wkv[deep, :], preferred_element_type=f32)

        load_wq.start()
        load_wo.start()
        own = kv_sum[...].astype(bf16)
        for i in range(blocks_here):
            kvbuf[0, i] = own[i * block_rows : (i + 1) * block_rows, :]

    with jax.named_scope("barrier"):
        pl.semaphore_wait(barrier, RING_Y + 2)

    def ring_copy(going_up, src_slot, dst_slot, c):
        view = pl.ds(c * BLOCKS_PER_CHUNK, BLOCKS_PER_CHUNK)
        step = dst_slot if going_up else ring_z - dst_slot
        return pltpu.make_async_remote_copy(
            src_ref=kvbuf.at[src_slot, view],
            dst_ref=kvbuf.at[dst_slot, view],
            send_sem=(plus_send if going_up else minus_send).at[0],
            recv_sem=(plus_recv if going_up else minus_recv).at[step - 1, c],
            device_id={"kv": up if going_up else down},
            device_id_type=MESH,
        )

    def sent(ref, sem, count):
        view = ref.at[pl.ds(0, count)]
        pltpu.make_async_remote_copy(
            src_ref=view,
            dst_ref=view,
            send_sem=sem,
            recv_sem=plus_recv.at[0, 0],
            device_id={"kv": up},
            device_id_type=MESH,
        ).wait_send()

    last_up, last_down = half - 2, half - 1

    def from_below(t):
        return (z >= t) & (t <= last_up)

    def to_above(t):
        return (z >= t) & (z < ring_z - 1) & (t < last_up)

    def from_above(t):
        return ((z + t) % ring_z <= last_down) & (t <= last_down)

    def to_below(t):
        source = (z + t) % ring_z
        return (source <= last_down) & (t < last_down)

    chosen_up = (z >= last_up) & (z < ring_z - 1)
    chosen_down = (z + last_down) % ring_z <= last_down

    with jax.named_scope("first_sends"):
        for c in range(chunks):

            @pl.when(to_above(0))
            def _():
                ring_copy(True, 0, 1, c).start()

            @pl.when(to_below(0))
            def _():
                ring_copy(False, 0, ring_z - 1, c).start()

    lanes = RING_Y * ring_z
    load_chosen.wait()
    lane = lax.broadcasted_iota(jnp.int32, (blocks_here, 128), 1)
    back_y, back_z = lane // ring_z, lane % ring_z
    source = ((z - back_z + ring_z) % ring_z) * RING_Y + (y - back_y + RING_Y) % RING_Y
    low = jnp.where(lane < lanes, source * blocks_here, me * blocks_here + lane - lanes)
    width = jnp.where(
        lane == 0,
        0,
        jnp.where(lane < lanes, blocks_here, jnp.where(lane < lanes + blocks_here, 1, 0)),
    )
    best = jnp.full((blocks_here, 128), -1, jnp.int32)
    picks = chosen[...].reshape(blocks_here, chosen.shape[2])
    for slot in range(chosen.shape[2]):
        inner = picks[:, slot : slot + 1] - low
        best = jnp.where((inner >= 0) & (inner < width), inner, best)
    mask_rows = jnp.where(best >= 0, 0.0, MASKED).astype(f32)
    want = jnp.maximum(best[0:1, :], 0)
    for i in range(1, blocks_here):
        want = jnp.maximum(want, best[i : i + 1, :])
    want_all[0] = want
    def want_copy(source, target, sem, peer):
        return pltpu.make_async_remote_copy(
            src_ref=want_all.at[source],
            dst_ref=want_all.at[target],
            send_sem=want_send.at[sem],
            recv_sem=want_recv.at[sem],
            device_id={"kv": peer},
            device_id_type=MESH,
        )

    row = pl.ds(0, RING_Y)
    rest = pl.ds(1, RING_Y - 1)
    want_side = want_copy(rest, rest, 0, up)
    want_up = want_copy(row, pl.ds(2 * RING_Y, RING_Y), 1, up)
    want_down = want_copy(row, pl.ds(RING_Y, RING_Y), 2, down)
    for d in (2, 1, 3):
        want_copy(0, RING_Y - d, 0, side[d]).start()

    for head in range(qx.shape[0] // rows):
        for i in range(blocks_here):
            qx[pl.ds(head * rows + i * block_rows, block_rows), HEAD_WIDTH:] = jnp.broadcast_to(
                mask_rows[i : i + 1, :], (block_rows, 128)
            ).astype(bf16)

    for slot in range(1, ring_z):

        @pl.when(z < slot)
        def _():
            table[slot] = jnp.zeros(table.shape[1:], bf16)

    with jax.named_scope("project_q"):
        load_wq.wait()
        queries = jnp.dot(tok[...], wq[...], preferred_element_type=f32).astype(bf16)
        heads = qx.shape[0] // rows
        for head in range(heads):
            qx[pl.ds(head * rows, rows), 0:HEAD_WIDTH] = queries[
                :, head * HEAD_WIDTH : (head + 1) * HEAD_WIDTH
            ]

    columns = qx.shape[0]
    tiles = columns // COLUMN_TILE

    def attend(tile, count, first):
        begin, size = (0, columns) if tile is None else (tile * COLUMN_TILE, COLUMN_TILE)
        here = pl.ds(begin, size)
        s = lax.dot_general(
            keys_in[0:count, :],
            qx[here, :],
            (((1,), (1,)), ((), ())),
            preferred_element_type=f32,
        ) * SCORE_SCALE
        if first:
            row = lax.broadcasted_iota(jnp.int32, s.shape, 1) + begin
            row = jnp.where(row >= rows, row - rows, row)
            s = jnp.where(lax.broadcasted_iota(jnp.int32, s.shape, 0) <= row, s, MASKED)
        top = jnp.max(s, axis=0, keepdims=True)
        if first:
            new_m = top
        else:
            old_m = m_ref[:, here]
            new_m = jnp.maximum(old_m, top)
            shrink = jnp.exp2(old_m - new_m)
        p = jnp.exp2(s - new_m)
        total = jnp.sum(p, axis=0, keepdims=True)
        summed = jnp.dot(values_in[:, 0:count], p.astype(bf16), preferred_element_type=f32)
        m_ref[:, here] = new_m
        if first:
            l_ref[:, here] = total
            acc[:, here] = summed
        else:
            l_ref[:, here] = l_ref[:, here] * shrink + total
            acc[:, here] = acc[:, here] * shrink + summed

    def attend_own():
        key_lane = lax.broadcasted_iota(jnp.int32, (rows, 128), 1)
        key_block = lax.broadcasted_iota(jnp.int32, (rows, 128), 0) // block_rows
        own_hot = jnp.where(key_lane == key_block + lanes, 1.0, 0.0).astype(bf16)
        own = kvbuf[0].reshape(rows, 2 * HEAD_WIDTH)
        keys_in[0:rows, 0:HEAD_WIDTH] = own[:, 0:HEAD_WIDTH]
        keys_in[0:rows, HEAD_WIDTH:] = own_hot
        values_in[:, 0:rows] = own[:, HEAD_WIDTH:].T
        attend(None, rows, True)

    def arrival(slot):
        return y_recv.at[jnp.where(slot > half + 1, ring_z - slot, slot)]

    def chosen_copy(d, slot, peer, kind):
        return pltpu.make_async_remote_copy(
            src_ref=outbox.at[slot, d],
            dst_ref=table.at[slot, d],
            send_sem=y_send.at[kind],
            recv_sem=arrival(slot),
            device_id={"kv": peer},
            device_id_type=MESH,
        )

    def arrived(slot, count, first):
        view = table.at[pl.ds(0, count), pl.ds(first, RING_Y - first)]
        pltpu.make_async_remote_copy(
            src_ref=view,
            dst_ref=view,
            send_sem=y_send.at[0],
            recv_sem=arrival(slot),
            device_id={"kv": up},
            device_id_type=MESH,
        ).wait_recv()

    def pass_on(slot):
        stage[...] = kvbuf[slot]
        for d in (2, 1, 3):
            outbox[slot, d] = stage[want_smem[d, 0, d * ring_z + slot]]
        table[slot, 0] = stage[want_smem[0, 0, slot]]
        for d in (2, 1, 3):
            chosen_copy(d, slot, side[d], 0).start()

    def pass_beyond(dz, held, slot):
        stage[...] = kvbuf[held]
        for d in (2, 1, 3, 0):
            row_there = (RING_Y if dz == 1 else 2 * RING_Y) + d
            outbox[slot, d] = stage[want_smem[row_there, 0, d * ring_z + slot]]
        for d in (2, 1, 3, 0):
            chosen_copy(d, slot, beyond[dz][d], 1 if dz == 1 else 2).start()

    near_keys = RING_Y * block_rows

    def attend_slots(tile, slots):
        if not tile:
            lane_row = lax.broadcasted_iota(jnp.int32, (near_keys, 128), 1)
            back = lax.broadcasted_iota(jnp.int32, (near_keys, 128), 0) // block_rows * ring_z
            for i, slot in enumerate(slots):
                both = table[slot].reshape(near_keys, 2 * HEAD_WIDTH)
                here = slice(i * near_keys, (i + 1) * near_keys)
                keys_in[here, 0:HEAD_WIDTH] = both[:, 0:HEAD_WIDTH]
                keys_in[here, HEAD_WIDTH:] = jnp.where(
                    lane_row == back + slot, 1.0, 0.0
                ).astype(bf16)
                values_in[:, here] = both[:, HEAD_WIDTH:].T
        attend(tile, len(slots) * near_keys, False)

    def due_from_above(t, c):
        behind = (t - 1) * chunks + c - (LAG[0] * (ring_z - 1 - z)) // LAG[1]
        m = jnp.maximum(behind, 0)
        crossed = z > last_down
        hops = jnp.where(crossed, m // chunks + ring_z - z, t)
        chunk = jnp.where(crossed, m % chunks, c)
        due = jnp.where(crossed, (behind >= 0) & (hops <= last_down), from_above(t))
        return due, hops, chunk

    def step(t, fill):
        for c in range(chunks):

            @pl.when(from_below(t))
            def _():
                ring_copy(True, t, t, c).wait_recv()

            @pl.when(to_above(t))
            def _():
                ring_copy(True, t, t + 1, c).start()

            due, hops, chunk = due_from_above(t, c)
            back = ring_z - hops

            @pl.when(due)
            def _():
                ring_copy(False, back, back, chunk).wait_recv()

            @pl.when(due & (hops < last_down))
            def _():
                ring_copy(False, back, back - 1, chunk).start()

            @pl.when(due & (chunk == chunks - 1) & (hops == last_down) & chosen_down)
            def _():
                pass_beyond(ring_z - 1, ring_z - last_down, half)

            @pl.when(due & (chunk == chunks - 1) & (z >= back))
            def _():
                pass_on(back)

            if c < chunks - 1:
                fill(c)

        if t is last_up:

            @pl.when(chosen_up)
            def _():
                pass_beyond(1, last_up, last_up + 1)

        if t is not last_down:

            @pl.when(z >= t)
            def _():
                pass_on(t)

        fill(chunks - 1)

    def near_slots(t):
        @pl.when((z >= t) & (z < ring_z - t))
        def _():
            arrived(t, 1, 1)

        @pl.when(z >= ring_z - t)
        def _():
            arrived(t, 2, 1)

    near_scalars = pltpu.make_async_copy(want_all.at[row], want_smem.at[row], load_sem.at[3])
    far_rows = pl.ds(RING_Y, 2 * RING_Y)
    far_scalars = pltpu.make_async_copy(want_all.at[far_rows], want_smem.at[far_rows], load_sem.at[3])

    def fill_first(c):
        if c == 1:
            want_side.wait()
            want_up.start()
            want_down.start()
            near_scalars.start()
        if c == chunks - 2:
            near_scalars.wait()
            pass_on(0)

    def fill_second(c):
        if c == chunks - 1:
            want_up.wait()
            want_down.wait()
            far_scalars.start()
            arrived(0, 1, 1)
            attend_slots(None, [0])
            far_scalars.wait()

    def fill_near(t, c):
        if c == 1:
            near_slots(t)
        for tile in {0: [], 1: [0], 2: [1, 2], 3: [3], 4: [4]}[c]:

            @pl.when(z >= t)
            def _():
                attend_slots(tile, [t, ring_z - t])

    share = pltpu.make_async_remote_copy(
        src_ref=attended,
        dst_ref=partner,
        send_sem=tp_send,
        recv_sem=tp_recv,
        device_id={"tp": 1 - core},
        device_id_type=MESH,
    )

    def finish():
        with jax.named_scope("normalise"):
            for tile in range(tiles):
                here = slice(tile * COLUMN_TILE, (tile + 1) * COLUMN_TILE)
                by_row[here, :] = (acc[:, here] / l_ref[:, here]).T.astype(bf16)
            for h in range(heads):
                attended[:, h * HEAD_WIDTH : (h + 1) * HEAD_WIDTH] = by_row[
                    h * rows : (h + 1) * rows, :
                ]
            load_wo.wait()
            share.start()
            width = heads * HEAD_WIDTH
            mine = pl.ds(pl.multiple_of(core * width, width), width)
            own_mixed[...] = jnp.dot(attended[...], wo[mine, :], preferred_element_type=f32)

        mass = m_ref[...] * LN_2 + jnp.log(l_ref[...])
        for h in range(heads):
            log_out[0, h : h + 1, :] = mass[:, h * rows : (h + 1) * rows]

    with jax.named_scope("own"):
        attend_own()
    with jax.named_scope("step_1"):
        step(1, fill_first)
    with jax.named_scope("step_2"):
        step(2, fill_second)

    @pl.loop(3, last_up)
    def _(t):
        with jax.named_scope("step_t"):
            step(t, functools.partial(fill_near, t - 2))

    @pl.when(z == 0)
    def _():
        finish()

    with jax.named_scope("step_6"):
        step(last_up, functools.partial(fill_near, last_up - 2))
    with jax.named_scope("step_7"):
        step(last_down, functools.partial(fill_near, last_down - 2))

    with jax.named_scope("last_but_one"):
        near_slots(last_up)

        @pl.when(z > last_up)
        def _():
            arrived(last_up + 1, 1, 0)

        @pl.when(z >= last_up)
        def _():
            attend_slots(None, [last_up, ring_z - last_up, last_up + 1])

    with jax.named_scope("last_wait"):

        @pl.when(z >= half)
        def _():
            arrived(half, 1, 0)

        @pl.when(z > half)
        def _():
            arrived(half + 1, 1, 1)

    with jax.named_scope("last"):

        @pl.when(z >= half)
        def _():
            attend_slots(None, [half, half + 1])

    @pl.when(z > 0)
    def _():
        finish()

    with jax.named_scope("sends"):
        ups = jnp.where(z < ring_z - 1, jnp.minimum(z + 1, last_up), 0)
        for n in range(1, last_up + 1):

            @pl.when(ups == n)
            def _():
                sent(kvbuf, plus_send.at[0], n)

        downs = jnp.where(
            z <= last_down,
            jnp.minimum(last_down + 1 - z, last_down),
            jnp.maximum(z - (ring_z - last_down), 0),
        )
        for n in range(1, last_down + 1):

            @pl.when(downs == n)
            def _():
                sent(kvbuf, minus_send.at[0], n)

        passes = jnp.minimum(z, last_up) + jnp.maximum(z - (ring_z - last_down - 1), 0) + 1
        for n in range(1, last_up + last_down + 2):

            @pl.when(passes == n)
            def _():
                sent(outbox.at[:, pl.ds(1, RING_Y - 1)], y_send.at[0], n)

        @pl.when(chosen_up)
        def _():
            sent(outbox, y_send.at[1], 1)

        @pl.when(chosen_down)
        def _():
            sent(outbox, y_send.at[2], 1)

    share.wait()


def mix_kernel(partner, wo, own_mixed, log_in, mixed_hbm, log_hbm, mixed, log_vmem, sem):
    width = partner.shape[1]
    other = 1 - lax.axis_index("tp")
    theirs = pl.ds(pl.multiple_of(other * width, width), width)
    log_vmem[...] = log_in[...]
    copies = [pltpu.make_async_copy(log_vmem, log_hbm, sem.at[0])]
    copies[0].start()
    step = wo.shape[1] // MIX_PARTS
    for i in range(MIX_PARTS):
        here = slice(i * step, (i + 1) * step)
        mixed[0, :, here] = (
            own_mixed[:, here]
            + jnp.dot(partner[...], wo[theirs, here], preferred_element_type=jnp.float32)
        ).astype(jnp.bfloat16)
        copy = pltpu.make_async_copy(
            mixed.at[:, :, pl.ds(i * step, step)], mixed_hbm.at[:, :, pl.ds(i * step, step)], sem.at[i + 1]
        )
        copy.start()
        copies.append(copy)
    for copy in copies:
        copy.wait()


def body(tokens, w_query, key_weight, value_weight, w_out, chosen):
    row_count, depth = tokens.shape[1], tokens.shape[2]
    blocks_here, slots = chosen.shape[1:]
    block_rows = row_count // blocks_here
    ring_z = lax.axis_size("kv") // RING_Y
    q_width = w_query.shape[1]
    heads = q_width // HEAD_WIDTH
    kv_width = key_weight.shape[1] + value_weight.shape[1]
    chunks = blocks_here // BLOCKS_PER_CHUNK
    dma = pltpu.SemaphoreType.DMA
    vmem = pltpu.VMEM
    hbm = lambda x: pltpu.with_memory_space_constraint(x, pltpu.HBM)
    partner, log_part, wo, own_mixed = pl.pallas_call(
        functools.partial(exchange_kernel, ring_z, blocks_here, block_rows),
        out_shape=(
            vmem((row_count, q_width), jnp.bfloat16),
            vmem((1, heads, row_count), jnp.float32),
            vmem(w_out.shape, jnp.bfloat16),
            vmem((row_count, w_out.shape[1]), jnp.float32),
        ),
        in_specs=[pl.BlockSpec(memory_space=pl.ANY)] * 6,
        out_specs=(pl.BlockSpec(memory_space=vmem),) * 4,
        scratch_shapes=[
            vmem((row_count, depth), jnp.bfloat16),
            vmem((depth, kv_width), jnp.bfloat16),
            vmem((depth, q_width), jnp.bfloat16),
            vmem((row_count, kv_width), jnp.float32),
            vmem((blocks_here, 1, slots), jnp.int32),
            vmem((ring_z, blocks_here, block_rows, kv_width), jnp.bfloat16),
            vmem((blocks_here, block_rows, kv_width), jnp.bfloat16),
            vmem((ring_z, RING_Y, block_rows, kv_width), jnp.bfloat16),
            vmem((ring_z, RING_Y, block_rows, kv_width), jnp.bfloat16),
            vmem((heads * row_count, 2 * HEAD_WIDTH), jnp.bfloat16),
            vmem((1, heads * row_count), jnp.float32),
            vmem((1, heads * row_count), jnp.float32),
            vmem((HEAD_WIDTH, heads * row_count), jnp.float32),
            vmem((max(row_count, 3 * RING_Y * block_rows), 2 * HEAD_WIDTH), jnp.bfloat16),
            vmem((HEAD_WIDTH, max(row_count, 3 * RING_Y * block_rows)), jnp.bfloat16),
            vmem((heads * row_count, HEAD_WIDTH), jnp.bfloat16),
            vmem((row_count, q_width), jnp.bfloat16),
            vmem((3 * RING_Y, 1, 128), jnp.int32),
            pltpu.SMEM((3 * RING_Y, 1, 128), jnp.int32),
            dma((4,)),
            dma((DEPTH_PARTS, 3)),
            dma((1,)),
            dma((ring_z // 2 - 2, chunks)),
            dma((1,)),
            dma((ring_z // 2 - 1, chunks)),
            dma((3,)),
            dma((ring_z // 2 + 2,)),
            dma((3,)),
            dma((3,)),
            dma,
            dma,
        ],
        compiler_params=pltpu.CompilerParams(
            collective_id=0, has_side_effects=True, vmem_limit_bytes=40 * 1024 * 1024
        ),
    )(*map(hbm, (tokens, w_query, key_weight, value_weight, w_out, chosen.reshape(blocks_here, 1, slots))))
    return pl.pallas_call(
        mix_kernel,
        out_shape=(
            jax.ShapeDtypeStruct((1, row_count, w_out.shape[1]), jnp.bfloat16),
            jax.ShapeDtypeStruct((1, heads, row_count), jnp.float32),
        ),
        in_specs=[pl.BlockSpec(memory_space=vmem)] * 4,
        out_specs=(pl.BlockSpec(memory_space=pl.ANY),) * 2,
        scratch_shapes=[
            vmem((1, row_count, w_out.shape[1]), jnp.bfloat16),
            vmem((1, heads, row_count), jnp.float32),
            dma((MIX_PARTS + 1,)),
        ],
        compiler_params=pltpu.CompilerParams(vmem_limit_bytes=12 * 1024 * 1024),
    )(partner, wo, own_mixed, log_part)


def solution(mesh):
    in_specs = (
        P("dp", "kv", None),
        P(None, "tp"),
        P(None, "tp"),
        P(None, "tp"),
        P(None, "tp"),
        P("dp", "kv", None),
    )
    out_specs = (P("dp", "kv", "tp"), P("dp", "tp", "kv"))
    return jax.shard_map(body, mesh=mesh, in_specs=in_specs, out_specs=out_specs, check_vma=False)
```

```python
import functools

import jax
import jax.numpy as jnp
from jax import lax
from jax.experimental import pallas as pl
from jax.experimental.pallas import tpu as pltpu
from jax.sharding import PartitionSpec as P

HEAD_WIDTH = 128
RING_Y = 4
BLOCKS_PER_CHUNK = 2
MASKED = -1e38
LOG2_E = 1.4426950408889634
LN_2 = 0.6931471805599453
SCORE_SCALE = HEAD_WIDTH ** (-0.5) * LOG2_E
MESH = pl.DeviceIdType.MESH
COLUMN_TILE = 128
DEPTH_PARTS = 2
MIX_PARTS = 4
LAG = (9, 2)


def exchange_kernel(
    ring_z,
    blocks_here,
    block_rows,
    tokens_hbm,
    wq_hbm,
    wk_hbm,
    wv_hbm,
    wo_hbm,
    chosen_hbm,
    partner,
    log_out,
    wo,
    own_mixed,
    tok,
    wkv,
    wq,
    kv_sum,
    chosen,
    kvbuf,
    stage,
    table,
    outbox,
    qx,
    m_ref,
    l_ref,
    acc,
    keys_in,
    values_in,
    by_row,
    attended,
    want_all,
    want_smem,
    load_sem,
    part_sem,
    plus_send,
    plus_recv,
    minus_send,
    minus_recv,
    y_send,
    y_recv,
    want_send,
    want_recv,
    tp_send,
    tp_recv,
):
    f32, bf16 = jnp.float32, jnp.bfloat16
    me = lax.axis_index("kv")
    core = lax.axis_index("tp")
    z, y = me // RING_Y, me % RING_Y
    rows = blocks_here * block_rows
    half = ring_z // 2
    wrap_last = half - 2
    chunks = blocks_here // BLOCKS_PER_CHUNK
    up = ((z + 1) % ring_z) * RING_Y + y
    down = ((z + ring_z - 1) % ring_z) * RING_Y + y

    side = [z * RING_Y + (y + d) % RING_Y for d in range(RING_Y)]
    beyond = {
        dz: [((z + dz) % ring_z) * RING_Y + (y + d) % RING_Y for d in range(RING_Y)]
        for dz in (1, ring_z - 1)
    }
    barrier = pltpu.get_barrier_semaphore()
    part_depth = tok.shape[1] // DEPTH_PARTS

    def loads_of(i):
        deep = pl.ds(pl.multiple_of(i * part_depth, part_depth), part_depth)
        k_lanes, v_lanes = pl.ds(0, HEAD_WIDTH), pl.ds(HEAD_WIDTH, HEAD_WIDTH)
        return [
            pltpu.make_async_copy(tokens_hbm.at[0, :, deep], tok.at[:, deep], part_sem.at[i, 0]),
            pltpu.make_async_copy(wk_hbm.at[deep], wkv.at[deep, k_lanes], part_sem.at[i, 1]),
            pltpu.make_async_copy(wv_hbm.at[deep], wkv.at[deep, v_lanes], part_sem.at[i, 2]),
        ]

    load_chosen = pltpu.make_async_copy(chosen_hbm, chosen, load_sem.at[0])
    load_wq = pltpu.make_async_copy(wq_hbm, wq, load_sem.at[1])
    load_wo = pltpu.make_async_copy(wo_hbm, wo, load_sem.at[2])
    for i in range(DEPTH_PARTS):
        for load in loads_of(i):
            load.start()
    load_chosen.start()
    for peer in [up, down] + side[1:]:
        pl.semaphore_signal(barrier, inc=1, device_id={"kv": peer}, device_id_type=MESH)
    pl.semaphore_signal(barrier, inc=1, device_id={"tp": 1 - core}, device_id_type=MESH)


    with jax.named_scope("project_kv"):
        kv_sum[...] = jnp.zeros_like(kv_sum)

        @pl.loop(0, DEPTH_PARTS)
        def _(i):
            for load in loads_of(i):
                load.wait()
            deep = pl.ds(pl.multiple_of(i * part_depth, part_depth), part_depth)
            kv_sum[...] += jnp.dot(tok[:, deep], wkv[deep, :], preferred_element_type=f32)

        load_wq.start()
        load_wo.start()
        own = kv_sum[...].astype(bf16)
        for i in range(blocks_here):
            kvbuf[0, i] = own[i * block_rows : (i + 1) * block_rows, :]

    with jax.named_scope("barrier"):
        pl.semaphore_wait(barrier, RING_Y + 2)

    def ring_arrival(going_up, step, c):
        sems, last_hop = (plus_recv, last_up) if going_up else (minus_recv, last_down)
        return sems.at[jnp.minimum((step - 1) * chunks + c, (last_hop - 1) * chunks)]

    def whole_slot(going_up, slot, step):
        return pltpu.make_async_remote_copy(
            src_ref=kvbuf.at[slot],
            dst_ref=kvbuf.at[slot],
            send_sem=(plus_send if going_up else minus_send).at[0],
            recv_sem=ring_arrival(going_up, step, 0),
            device_id={"kv": up},
            device_id_type=MESH,
        )

    def ring_copy(going_up, src_slot, dst_slot, c):
        view = pl.ds(c * BLOCKS_PER_CHUNK, BLOCKS_PER_CHUNK)
        step = dst_slot if going_up else ring_z - dst_slot
        return pltpu.make_async_remote_copy(
            src_ref=kvbuf.at[src_slot, view],
            dst_ref=kvbuf.at[dst_slot, view],
            send_sem=(plus_send if going_up else minus_send).at[0],
            recv_sem=ring_arrival(going_up, step, c),
            device_id={"kv": up if going_up else down},
            device_id_type=MESH,
        )

    def sent(ref, sem, count):
        view = ref.at[pl.ds(0, count)]
        pltpu.make_async_remote_copy(
            src_ref=view,
            dst_ref=view,
            send_sem=sem,
            recv_sem=plus_recv.at[0],
            device_id={"kv": up},
            device_id_type=MESH,
        ).wait_send()

    last_up, last_down = half - 2, half - 1

    def from_below(t):
        return (z >= t) & (t <= last_up)

    def to_above(t):
        return (z >= t) & (z < ring_z - 1) & (t < last_up)

    def from_above(t):
        return ((z + t) % ring_z <= last_down) & (t <= last_down)

    def to_below(t):
        source = (z + t) % ring_z
        return (source <= last_down) & (t < last_down)

    chosen_up = (z >= last_up) & (z < ring_z - 1)
    chosen_down = (z + last_down) % ring_z <= last_down

    with jax.named_scope("first_sends"):
        for c in range(chunks):

            @pl.when(to_above(0))
            def _():
                ring_copy(True, 0, 1, c).start()

            @pl.when(to_below(0))
            def _():
                ring_copy(False, 0, ring_z - 1, c).start()

    lanes = RING_Y * ring_z
    load_chosen.wait()
    lane = lax.broadcasted_iota(jnp.int32, (blocks_here, 128), 1)
    back_y, back_z = lane // ring_z, lane % ring_z
    source = ((z - back_z + ring_z) % ring_z) * RING_Y + (y - back_y + RING_Y) % RING_Y
    low = jnp.where(lane < lanes, source * blocks_here, me * blocks_here + lane - lanes)
    width = jnp.where(
        lane == 0,
        0,
        jnp.where(lane < lanes, blocks_here, jnp.where(lane < lanes + blocks_here, 1, 0)),
    )
    best = jnp.full((blocks_here, 128), -1, jnp.int32)
    picks = chosen[...].reshape(blocks_here, chosen.shape[2])
    for slot in range(chosen.shape[2]):
        inner = picks[:, slot : slot + 1] - low
        best = jnp.where((inner >= 0) & (inner < width), inner, best)
    mask_rows = jnp.where(best >= 0, 0.0, MASKED).astype(f32)
    want = jnp.maximum(best[0:1, :], 0)
    for i in range(1, blocks_here):
        want = jnp.maximum(want, best[i : i + 1, :])
    want_all[0] = want
    def want_copy(source, target, sem, peer):
        return pltpu.make_async_remote_copy(
            src_ref=want_all.at[source],
            dst_ref=want_all.at[target],
            send_sem=want_send.at[sem],
            recv_sem=want_recv.at[sem],
            device_id={"kv": peer},
            device_id_type=MESH,
        )

    row = pl.ds(0, RING_Y)
    rest = pl.ds(1, RING_Y - 1)
    want_side = want_copy(rest, rest, 0, up)
    want_up = want_copy(row, pl.ds(2 * RING_Y, RING_Y), 1, up)
    want_down = want_copy(row, pl.ds(RING_Y, RING_Y), 2, down)
    for d in (2, 1, 3):
        want_copy(0, RING_Y - d, 0, side[d]).start()

    for head in range(qx.shape[0] // rows):
        for i in range(blocks_here):
            qx[pl.ds(head * rows + i * block_rows, block_rows), HEAD_WIDTH:] = jnp.broadcast_to(
                mask_rows[i : i + 1, :], (block_rows, 128)
            ).astype(bf16)

    for slot in range(1, ring_z):

        @pl.when(z < slot)
        def _():
            table[slot] = jnp.zeros(table.shape[1:], bf16)

    with jax.named_scope("project_q"):
        load_wq.wait()
        queries = jnp.dot(tok[...], wq[...], preferred_element_type=f32).astype(bf16)
        heads = qx.shape[0] // rows
        for head in range(heads):
            qx[pl.ds(head * rows, rows), 0:HEAD_WIDTH] = queries[
                :, head * HEAD_WIDTH : (head + 1) * HEAD_WIDTH
            ]

    columns = qx.shape[0]
    tiles = columns // COLUMN_TILE

    def attend(tile, count, first):
        begin, size = (0, columns) if tile is None else tile
        here = pl.ds(begin, size)
        s = lax.dot_general(
            keys_in[0:count, :],
            qx[here, :],
            (((1,), (1,)), ((), ())),
            preferred_element_type=f32,
        ) * SCORE_SCALE
        if first:
            row = lax.broadcasted_iota(jnp.int32, s.shape, 1) + begin
            row = jnp.where(row >= rows, row - rows, row)
            s = jnp.where(lax.broadcasted_iota(jnp.int32, s.shape, 0) <= row, s, MASKED)
        top = jnp.max(s, axis=0, keepdims=True)
        if first:
            new_m = top
        else:
            old_m = m_ref[:, here]
            new_m = jnp.maximum(old_m, top)
            shrink = jnp.exp2(old_m - new_m)
        p = jnp.exp2(s - new_m)
        total = jnp.sum(p, axis=0, keepdims=True)
        summed = jnp.dot(values_in[:, 0:count], p.astype(bf16), preferred_element_type=f32)
        m_ref[:, here] = new_m
        if first:
            l_ref[:, here] = total
            acc[:, here] = summed
        else:
            l_ref[:, here] = l_ref[:, here] * shrink + total
            acc[:, here] = acc[:, here] * shrink + summed

    def attend_own():
        key_lane = lax.broadcasted_iota(jnp.int32, (rows, 128), 1)
        key_block = lax.broadcasted_iota(jnp.int32, (rows, 128), 0) // block_rows
        own_hot = jnp.where(key_lane == key_block + lanes, 1.0, 0.0).astype(bf16)
        own = kvbuf[0].reshape(rows, 2 * HEAD_WIDTH)
        keys_in[0:rows, 0:HEAD_WIDTH] = own[:, 0:HEAD_WIDTH]
        keys_in[0:rows, HEAD_WIDTH:] = own_hot
        values_in[:, 0:rows] = own[:, HEAD_WIDTH:].T
        attend(None, rows, True)

    def arrival(slot):
        return y_recv.at[jnp.where(slot > half + 1, ring_z - slot, slot)]

    def chosen_copy(d, slot, peer, kind):
        return pltpu.make_async_remote_copy(
            src_ref=outbox.at[slot, d],
            dst_ref=table.at[slot, d],
            send_sem=y_send.at[kind],
            recv_sem=arrival(slot),
            device_id={"kv": peer},
            device_id_type=MESH,
        )

    def arrived(slot, count, first):
        view = table.at[pl.ds(0, count), pl.ds(first, RING_Y - first)]
        pltpu.make_async_remote_copy(
            src_ref=view,
            dst_ref=view,
            send_sem=y_send.at[0],
            recv_sem=arrival(slot),
            device_id={"kv": up},
            device_id_type=MESH,
        ).wait_recv()

    def pass_on(slot):
        stage[...] = kvbuf[slot]
        for d in (2, 1, 3):
            outbox[slot, d] = stage[want_smem[d, 0, d * ring_z + slot]]
        table[slot, 0] = stage[want_smem[0, 0, slot]]
        for d in (2, 1, 3):
            chosen_copy(d, slot, side[d], 0).start()

    def pass_beyond(dz, held, slot):
        stage[...] = kvbuf[held]
        for d in (2, 1, 3, 0):
            row_there = (RING_Y if dz == 1 else 2 * RING_Y) + d
            outbox[slot, d] = stage[want_smem[row_there, 0, d * ring_z + slot]]
        for d in (2, 1, 3, 0):
            chosen_copy(d, slot, beyond[dz][d], 1 if dz == 1 else 2).start()

    near_keys = RING_Y * block_rows

    def attend_slots(tile, slots):
        if tile is None or tile[0] == 0:
            lane_row = lax.broadcasted_iota(jnp.int32, (near_keys, 128), 1)
            back = lax.broadcasted_iota(jnp.int32, (near_keys, 128), 0) // block_rows * ring_z
            for i, slot in enumerate(slots):
                both = table[slot].reshape(near_keys, 2 * HEAD_WIDTH)
                here = slice(i * near_keys, (i + 1) * near_keys)
                keys_in[here, 0:HEAD_WIDTH] = both[:, 0:HEAD_WIDTH]
                keys_in[here, HEAD_WIDTH:] = jnp.where(
                    lane_row == back + slot, 1.0, 0.0
                ).astype(bf16)
                values_in[:, here] = both[:, HEAD_WIDTH:].T
        attend(tile, len(slots) * near_keys, False)

    def due_from_above(t, c):
        behind = (t - 1) * chunks + c - (LAG[0] * (ring_z - 1 - z)) // LAG[1]
        m = jnp.maximum(behind, 0)
        crossed = z > last_down
        hops = jnp.where(crossed, m // chunks + ring_z - z, t)
        chunk = jnp.where(crossed, m % chunks, c)
        due = jnp.where(crossed, (behind >= 0) & (hops <= last_down), from_above(t))
        return due, hops, chunk

    def step(t, fill):
        for c in range(chunks):

            if t is not last_up:

                @pl.when(from_below(t))
                def _():
                    ring_copy(True, t, t, c).wait_recv()

            elif c == chunks - 1:

                @pl.when(from_below(t))
                def _():
                    whole_slot(True, t, t).wait_recv()

            @pl.when(to_above(t))
            def _():
                ring_copy(True, t, t + 1, c).start()

            due, hops, chunk = due_from_above(t, c)
            back = ring_z - hops

            @pl.when(due & (hops < last_down))
            def _():
                ring_copy(False, back, back, chunk).wait_recv()

            @pl.when(due & (hops == last_down) & (chunk == chunks - 1))
            def _():
                whole_slot(False, ring_z - last_down, last_down).wait_recv()

            @pl.when(due & (hops < last_down))
            def _():
                ring_copy(False, back, back - 1, chunk).start()

            @pl.when(due & (chunk == chunks - 1) & (hops == last_down) & chosen_down)
            def _():
                pass_beyond(ring_z - 1, ring_z - last_down, half)

            @pl.when(due & (chunk == chunks - 1) & (z >= back))
            def _():
                pass_on(back)

            if c < chunks - 1:
                fill(c)

        if t is last_up:

            @pl.when(chosen_up)
            def _():
                pass_beyond(1, last_up, last_up + 1)

        if t is not last_down:

            @pl.when(z >= t)
            def _():
                pass_on(t)

        fill(chunks - 1)

    def near_slots(t):
        @pl.when((z >= t) & (z < ring_z - t))
        def _():
            arrived(t, 1, 1)

        @pl.when(z >= ring_z - t)
        def _():
            arrived(t, 2, 1)

    near_scalars = pltpu.make_async_copy(want_all.at[row], want_smem.at[row], load_sem.at[3])
    far_rows = pl.ds(RING_Y, 2 * RING_Y)
    far_scalars = pltpu.make_async_copy(want_all.at[far_rows], want_smem.at[far_rows], load_sem.at[3])

    def fill_first(c):
        if c == 1:
            want_side.wait()
            want_up.start()
            want_down.start()
            near_scalars.start()
        if c == chunks - 2:
            near_scalars.wait()
            pass_on(0)

    def fill_second(c):
        if c == chunks - 1:
            want_up.wait()
            want_down.wait()
            far_scalars.start()
            arrived(0, 1, 1)
            attend_slots(None, [0])
            far_scalars.wait()

    def fill_near(t, c):
        if c == 1:
            near_slots(t)
        wide = 3 * COLUMN_TILE
        for tile in {1: [(0, wide)], 3: [(wide, columns - wide)]}.get(c, []):

            @pl.when(z >= t)
            def _():
                attend_slots(tile, [t, ring_z - t])

    share = pltpu.make_async_remote_copy(
        src_ref=attended,
        dst_ref=partner,
        send_sem=tp_send,
        recv_sem=tp_recv,
        device_id={"tp": 1 - core},
        device_id_type=MESH,
    )

    def finish():
        with jax.named_scope("normalise"):
            for tile in range(tiles):
                here = slice(tile * COLUMN_TILE, (tile + 1) * COLUMN_TILE)
                by_row[here, :] = (acc[:, here] / l_ref[:, here]).T.astype(bf16)
            for h in range(heads):
                attended[:, h * HEAD_WIDTH : (h + 1) * HEAD_WIDTH] = by_row[
                    h * rows : (h + 1) * rows, :
                ]
            load_wo.wait()
            share.start()
            width = heads * HEAD_WIDTH
            mine = pl.ds(pl.multiple_of(core * width, width), width)
            own_mixed[...] = jnp.dot(attended[...], wo[mine, :], preferred_element_type=f32)

        mass = m_ref[...] * LN_2 + jnp.log(l_ref[...])
        for h in range(heads):
            log_out[0, h : h + 1, :] = mass[:, h * rows : (h + 1) * rows]

    with jax.named_scope("own"):
        attend_own()
    with jax.named_scope("step_1"):
        step(1, fill_first)
    with jax.named_scope("step_2"):
        step(2, fill_second)

    @pl.loop(3, last_up)
    def _(t):
        with jax.named_scope("step_t"):
            step(t, functools.partial(fill_near, t - 2))

    @pl.when(z == 0)
    def _():
        finish()

    with jax.named_scope("step_6"):
        step(last_up, functools.partial(fill_near, last_up - 2))
    with jax.named_scope("step_7"):
        step(last_down, functools.partial(fill_near, last_down - 2))

    with jax.named_scope("last_but_one"):
        near_slots(last_up)

        @pl.when(z > last_up)
        def _():
            arrived(last_up + 1, 1, 0)

        @pl.when(z >= last_up)
        def _():
            attend_slots(None, [last_up, ring_z - last_up, last_up + 1])

    with jax.named_scope("last_wait"):

        @pl.when(z >= half)
        def _():
            arrived(half, 1, 0)

        @pl.when(z > half)
        def _():
            arrived(half + 1, 1, 1)

    with jax.named_scope("last"):

        @pl.when(z >= half)
        def _():
            attend_slots(None, [half, half + 1])

    @pl.when(z > 0)
    def _():
        finish()

    with jax.named_scope("sends"):
        ups = jnp.where(z < ring_z - 1, jnp.minimum(z + 1, last_up), 0)
        for n in range(1, last_up + 1):

            @pl.when(ups == n)
            def _():
                sent(kvbuf, plus_send.at[0], n)

        downs = jnp.where(
            z <= last_down,
            jnp.minimum(last_down + 1 - z, last_down),
            jnp.maximum(z - (ring_z - last_down), 0),
        )
        for n in range(1, last_down + 1):

            @pl.when(downs == n)
            def _():
                sent(kvbuf, minus_send.at[0], n)

        passes = jnp.minimum(z, last_up) + jnp.maximum(z - (ring_z - last_down - 1), 0) + 1
        for n in range(1, last_up + last_down + 2):

            @pl.when(passes == n)
            def _():
                sent(outbox.at[:, pl.ds(1, RING_Y - 1)], y_send.at[0], n)

        @pl.when(chosen_up)
        def _():
            sent(outbox, y_send.at[1], 1)

        @pl.when(chosen_down)
        def _():
            sent(outbox, y_send.at[2], 1)

    share.wait()


def mix_kernel(partner, wo, own_mixed, log_in, mixed_hbm, log_hbm, mixed, log_vmem, sem):
    width = partner.shape[1]
    other = 1 - lax.axis_index("tp")
    theirs = pl.ds(pl.multiple_of(other * width, width), width)
    log_vmem[...] = log_in[...]
    copies = [pltpu.make_async_copy(log_vmem, log_hbm, sem.at[0])]
    copies[0].start()
    step = wo.shape[1] // MIX_PARTS
    for i in range(MIX_PARTS):
        here = slice(i * step, (i + 1) * step)
        mixed[0, :, here] = (
            own_mixed[:, here]
            + jnp.dot(partner[...], wo[theirs, here], preferred_element_type=jnp.float32)
        ).astype(jnp.bfloat16)
        copy = pltpu.make_async_copy(
            mixed.at[:, :, pl.ds(i * step, step)], mixed_hbm.at[:, :, pl.ds(i * step, step)], sem.at[i + 1]
        )
        copy.start()
        copies.append(copy)
    for copy in copies:
        copy.wait()


def body(tokens, w_query, key_weight, value_weight, w_out, chosen):
    row_count, depth = tokens.shape[1], tokens.shape[2]
    blocks_here, slots = chosen.shape[1:]
    block_rows = row_count // blocks_here
    ring_z = lax.axis_size("kv") // RING_Y
    q_width = w_query.shape[1]
    heads = q_width // HEAD_WIDTH
    kv_width = key_weight.shape[1] + value_weight.shape[1]
    chunks = blocks_here // BLOCKS_PER_CHUNK
    dma = pltpu.SemaphoreType.DMA
    vmem = pltpu.VMEM
    hbm = lambda x: pltpu.with_memory_space_constraint(x, pltpu.HBM)
    partner, log_part, wo, own_mixed = pl.pallas_call(
        functools.partial(exchange_kernel, ring_z, blocks_here, block_rows),
        out_shape=(
            vmem((row_count, q_width), jnp.bfloat16),
            vmem((1, heads, row_count), jnp.float32),
            vmem(w_out.shape, jnp.bfloat16),
            vmem((row_count, w_out.shape[1]), jnp.float32),
        ),
        in_specs=[pl.BlockSpec(memory_space=pl.ANY)] * 6,
        out_specs=(pl.BlockSpec(memory_space=vmem),) * 4,
        scratch_shapes=[
            vmem((row_count, depth), jnp.bfloat16),
            vmem((depth, kv_width), jnp.bfloat16),
            vmem((depth, q_width), jnp.bfloat16),
            vmem((row_count, kv_width), jnp.float32),
            vmem((blocks_here, 1, slots), jnp.int32),
            vmem((ring_z, blocks_here, block_rows, kv_width), jnp.bfloat16),
            vmem((blocks_here, block_rows, kv_width), jnp.bfloat16),
            vmem((ring_z, RING_Y, block_rows, kv_width), jnp.bfloat16),
            vmem((ring_z, RING_Y, block_rows, kv_width), jnp.bfloat16),
            vmem((heads * row_count, 2 * HEAD_WIDTH), jnp.bfloat16),
            vmem((1, heads * row_count), jnp.float32),
            vmem((1, heads * row_count), jnp.float32),
            vmem((HEAD_WIDTH, heads * row_count), jnp.float32),
            vmem((max(row_count, 3 * RING_Y * block_rows), 2 * HEAD_WIDTH), jnp.bfloat16),
            vmem((HEAD_WIDTH, max(row_count, 3 * RING_Y * block_rows)), jnp.bfloat16),
            vmem((heads * row_count, HEAD_WIDTH), jnp.bfloat16),
            vmem((row_count, q_width), jnp.bfloat16),
            vmem((3 * RING_Y, 1, 128), jnp.int32),
            pltpu.SMEM((3 * RING_Y, 1, 128), jnp.int32),
            dma((4,)),
            dma((DEPTH_PARTS, 3)),
            dma((1,)),
            dma(((ring_z // 2 - 3) * chunks + 1,)),
            dma((1,)),
            dma(((ring_z // 2 - 2) * chunks + 1,)),
            dma((3,)),
            dma((ring_z // 2 + 2,)),
            dma((3,)),
            dma((3,)),
            dma,
            dma,
        ],
        compiler_params=pltpu.CompilerParams(
            collective_id=0, has_side_effects=True, vmem_limit_bytes=40 * 1024 * 1024
        ),
    )(*map(hbm, (tokens, w_query, key_weight, value_weight, w_out, chosen.reshape(blocks_here, 1, slots))))
    return pl.pallas_call(
        mix_kernel,
        out_shape=(
            jax.ShapeDtypeStruct((1, row_count, w_out.shape[1]), jnp.bfloat16),
            jax.ShapeDtypeStruct((1, heads, row_count), jnp.float32),
        ),
        in_specs=[pl.BlockSpec(memory_space=vmem)] * 4,
        out_specs=(pl.BlockSpec(memory_space=pl.ANY),) * 2,
        scratch_shapes=[
            vmem((1, row_count, w_out.shape[1]), jnp.bfloat16),
            vmem((1, heads, row_count), jnp.float32),
            dma((MIX_PARTS + 1,)),
        ],
        compiler_params=pltpu.CompilerParams(vmem_limit_bytes=12 * 1024 * 1024),
    )(partner, wo, own_mixed, log_part)


def solution(mesh):
    in_specs = (
        P("dp", "kv", None),
        P(None, "tp"),
        P(None, "tp"),
        P(None, "tp"),
        P(None, "tp"),
        P("dp", "kv", None),
    )
    out_specs = (P("dp", "kv", "tp"), P("dp", "tp", "kv"))
    return jax.shard_map(body, mesh=mesh, in_specs=in_specs, out_specs=out_specs, check_vma=False)
```

```python
import functools

import jax
import jax.numpy as jnp
from jax import lax
from jax.experimental import pallas as pl
from jax.experimental.pallas import tpu as pltpu
from jax.sharding import PartitionSpec as P

HEAD_WIDTH = 128
RING_Y = 4
BLOCKS_PER_CHUNK = 2
MASKED = -1e38
LOG2_E = 1.4426950408889634
LN_2 = 0.6931471805599453
SCORE_SCALE = HEAD_WIDTH ** (-0.5) * LOG2_E
MESH = pl.DeviceIdType.MESH
COLUMN_TILE = 128
DEPTH_PARTS = 2
MIX_PARTS = 4
LAG = (9, 2)


def exchange_kernel(
    ring_z,
    blocks_here,
    block_rows,
    tokens_hbm,
    wq_hbm,
    wk_hbm,
    wv_hbm,
    wo_hbm,
    chosen_hbm,
    partner,
    log_out,
    wo,
    own_mixed,
    tok,
    wkv,
    wq,
    kv_sum,
    chosen,
    kvbuf,
    stage,
    table,
    outbox,
    qx,
    m_ref,
    l_ref,
    acc,
    keys_in,
    values_in,
    by_row,
    attended,
    want_all,
    want_smem,
    load_sem,
    part_sem,
    plus_send,
    plus_recv,
    minus_send,
    minus_recv,
    y_send,
    y_recv,
    want_send,
    want_recv,
    tp_send,
    tp_recv,
):
    f32, bf16 = jnp.float32, jnp.bfloat16
    me = lax.axis_index("kv")
    core = lax.axis_index("tp")
    z, y = me // RING_Y, me % RING_Y
    rows = blocks_here * block_rows
    half = ring_z // 2
    wrap_last = half - 2
    chunks = blocks_here // BLOCKS_PER_CHUNK
    up = ((z + 1) % ring_z) * RING_Y + y
    down = ((z + ring_z - 1) % ring_z) * RING_Y + y

    side = [z * RING_Y + (y + d) % RING_Y for d in range(RING_Y)]
    beyond = {
        dz: [((z + dz) % ring_z) * RING_Y + (y + d) % RING_Y for d in range(RING_Y)]
        for dz in (1, ring_z - 1)
    }
    barrier = pltpu.get_barrier_semaphore()
    part_depth = tok.shape[1] // DEPTH_PARTS

    def loads_of(i):
        deep = pl.ds(pl.multiple_of(i * part_depth, part_depth), part_depth)
        k_lanes, v_lanes = pl.ds(0, HEAD_WIDTH), pl.ds(HEAD_WIDTH, HEAD_WIDTH)
        return [
            pltpu.make_async_copy(tokens_hbm.at[0, :, deep], tok.at[:, deep], part_sem.at[i, 0]),
            pltpu.make_async_copy(wk_hbm.at[deep], wkv.at[deep, k_lanes], part_sem.at[i, 1]),
            pltpu.make_async_copy(wv_hbm.at[deep], wkv.at[deep, v_lanes], part_sem.at[i, 1]),
        ]

    load_chosen = pltpu.make_async_copy(chosen_hbm, chosen, load_sem.at[0])
    load_wq = pltpu.make_async_copy(wq_hbm, wq, load_sem.at[1])
    load_wo = pltpu.make_async_copy(wo_hbm, wo, load_sem.at[2])
    for i in range(DEPTH_PARTS):
        for load in loads_of(i):
            load.start()
    load_chosen.start()
    for peer in [up, down] + side[1:]:
        pl.semaphore_signal(barrier, inc=1, device_id={"kv": peer}, device_id_type=MESH)
    pl.semaphore_signal(barrier, inc=1, device_id={"tp": 1 - core}, device_id_type=MESH)


    with jax.named_scope("project_kv"):
        kv_sum[...] = jnp.zeros_like(kv_sum)

        @pl.loop(0, DEPTH_PARTS)
        def _(i):
            deep = pl.ds(pl.multiple_of(i * part_depth, part_depth), part_depth)
            loads_of(i)[0].wait()
            both = wkv.at[deep]
            pltpu.make_async_copy(both, both, part_sem.at[i, 1]).wait()
            kv_sum[...] += jnp.dot(tok[:, deep], wkv[deep, :], preferred_element_type=f32)

        load_wq.start()
        load_wo.start()
        own = kv_sum[...].astype(bf16)
        for i in range(blocks_here):
            kvbuf[0, i] = own[i * block_rows : (i + 1) * block_rows, :]

    with jax.named_scope("barrier"):
        pl.semaphore_wait(barrier, RING_Y + 2)

    def ring_arrival(going_up, step, c):
        sems, last_hop = (plus_recv, last_up) if going_up else (minus_recv, last_down)
        return sems.at[jnp.minimum((step - 1) * chunks + c, (last_hop - 1) * chunks)]

    def whole_slot(going_up, slot, step):
        return pltpu.make_async_remote_copy(
            src_ref=kvbuf.at[slot],
            dst_ref=kvbuf.at[slot],
            send_sem=(plus_send if going_up else minus_send).at[0],
            recv_sem=ring_arrival(going_up, step, 0),
            device_id={"kv": up},
            device_id_type=MESH,
        )

    def ring_copy(going_up, src_slot, dst_slot, c):
        view = pl.ds(c * BLOCKS_PER_CHUNK, BLOCKS_PER_CHUNK)
        step = dst_slot if going_up else ring_z - dst_slot
        return pltpu.make_async_remote_copy(
            src_ref=kvbuf.at[src_slot, view],
            dst_ref=kvbuf.at[dst_slot, view],
            send_sem=(plus_send if going_up else minus_send).at[0],
            recv_sem=ring_arrival(going_up, step, c),
            device_id={"kv": up if going_up else down},
            device_id_type=MESH,
        )

    def sent(ref, sem, count):
        view = ref.at[pl.ds(0, count)]
        pltpu.make_async_remote_copy(
            src_ref=view,
            dst_ref=view,
            send_sem=sem,
            recv_sem=plus_recv.at[0],
            device_id={"kv": up},
            device_id_type=MESH,
        ).wait_send()

    last_up, last_down = half - 2, half - 1

    def from_below(t):
        return (z >= t) & (t <= last_up)

    def to_above(t):
        return (z >= t) & (z < ring_z - 1) & (t < last_up)

    def from_above(t):
        return ((z + t) % ring_z <= last_down) & (t <= last_down)

    def to_below(t):
        source = (z + t) % ring_z
        return (source <= last_down) & (t < last_down)

    chosen_up = (z >= last_up) & (z < ring_z - 1)
    chosen_down = (z + last_down) % ring_z <= last_down

    with jax.named_scope("first_sends"):
        for c in range(chunks):

            @pl.when(to_above(0))
            def _():
                ring_copy(True, 0, 1, c).start()

            @pl.when(to_below(0))
            def _():
                ring_copy(False, 0, ring_z - 1, c).start()

    lanes = RING_Y * ring_z
    load_chosen.wait()
    lane = lax.broadcasted_iota(jnp.int32, (blocks_here, 128), 1)
    back_y, back_z = lane // ring_z, lane % ring_z
    source = ((z - back_z + ring_z) % ring_z) * RING_Y + (y - back_y + RING_Y) % RING_Y
    low = jnp.where(lane < lanes, source * blocks_here, me * blocks_here + lane - lanes)
    width = jnp.where(
        lane == 0,
        0,
        jnp.where(lane < lanes, blocks_here, jnp.where(lane < lanes + blocks_here, 1, 0)),
    )
    best = jnp.full((blocks_here, 128), -1, jnp.int32)
    picks = chosen[...].reshape(blocks_here, chosen.shape[2])
    for slot in range(chosen.shape[2]):
        inner = picks[:, slot : slot + 1] - low
        best = jnp.where((inner >= 0) & (inner < width), inner, best)
    mask_rows = jnp.where(best >= 0, 0.0, MASKED).astype(f32)
    want = jnp.maximum(best[0:1, :], 0)
    for i in range(1, blocks_here):
        want = jnp.maximum(want, best[i : i + 1, :])
    want_all[0] = want
    def want_copy(source, target, sem, peer):
        return pltpu.make_async_remote_copy(
            src_ref=want_all.at[source],
            dst_ref=want_all.at[target],
            send_sem=want_send.at[sem],
            recv_sem=want_recv.at[sem],
            device_id={"kv": peer},
            device_id_type=MESH,
        )

    row = pl.ds(0, RING_Y)
    rest = pl.ds(1, RING_Y - 1)
    want_side = want_copy(rest, rest, 0, up)
    want_up = want_copy(row, pl.ds(2 * RING_Y, RING_Y), 1, up)
    want_down = want_copy(row, pl.ds(RING_Y, RING_Y), 2, down)
    for d in (2, 1, 3):
        want_copy(0, RING_Y - d, 0, side[d]).start()

    for head in range(qx.shape[0] // rows):
        for i in range(blocks_here):
            qx[pl.ds(head * rows + i * block_rows, block_rows), HEAD_WIDTH:] = jnp.broadcast_to(
                mask_rows[i : i + 1, :], (block_rows, 128)
            ).astype(bf16)

    for slot in range(1, ring_z):

        @pl.when(z < slot)
        def _():
            table[slot] = jnp.zeros(table.shape[1:], bf16)

    with jax.named_scope("project_q"):
        load_wq.wait()
        queries = jnp.dot(tok[...], wq[...], preferred_element_type=f32).astype(bf16)
        heads = qx.shape[0] // rows
        for head in range(heads):
            qx[pl.ds(head * rows, rows), 0:HEAD_WIDTH] = queries[
                :, head * HEAD_WIDTH : (head + 1) * HEAD_WIDTH
            ]

    columns = qx.shape[0]
    tiles = columns // COLUMN_TILE

    def attend(tile, count, first):
        begin, size = (0, columns) if tile is None else tile
        here = pl.ds(begin, size)
        s = lax.dot_general(
            keys_in[0:count, :],
            qx[here, :],
            (((1,), (1,)), ((), ())),
            preferred_element_type=f32,
        ) * SCORE_SCALE
        if first:
            row = lax.broadcasted_iota(jnp.int32, s.shape, 1) + begin
            row = jnp.where(row >= rows, row - rows, row)
            s = jnp.where(lax.broadcasted_iota(jnp.int32, s.shape, 0) <= row, s, MASKED)
        top = jnp.max(s, axis=0, keepdims=True)
        if first:
            new_m = top
        else:
            old_m = m_ref[:, here]
            new_m = jnp.maximum(old_m, top)
            shrink = jnp.exp2(old_m - new_m)
        p = jnp.exp2(s - new_m)
        total = jnp.sum(p, axis=0, keepdims=True)
        summed = jnp.dot(values_in[:, 0:count], p.astype(bf16), preferred_element_type=f32)
        m_ref[:, here] = new_m
        if first:
            l_ref[:, here] = total
            acc[:, here] = summed
        else:
            l_ref[:, here] = l_ref[:, here] * shrink + total
            acc[:, here] = acc[:, here] * shrink + summed

    def attend_own():
        key_lane = lax.broadcasted_iota(jnp.int32, (rows, 128), 1)
        key_block = lax.broadcasted_iota(jnp.int32, (rows, 128), 0) // block_rows
        own_hot = jnp.where(key_lane == key_block + lanes, 1.0, 0.0).astype(bf16)
        own = kvbuf[0].reshape(rows, 2 * HEAD_WIDTH)
        keys_in[0:rows, 0:HEAD_WIDTH] = own[:, 0:HEAD_WIDTH]
        keys_in[0:rows, HEAD_WIDTH:] = own_hot
        values_in[:, 0:rows] = own[:, HEAD_WIDTH:].T
        attend(None, rows, True)

    def arrival(slot):
        return y_recv.at[jnp.where(slot > half + 1, ring_z - slot, slot)]

    def chosen_copy(d, slot, peer, kind):
        return pltpu.make_async_remote_copy(
            src_ref=outbox.at[slot, d],
            dst_ref=table.at[slot, d],
            send_sem=y_send.at[kind],
            recv_sem=arrival(slot),
            device_id={"kv": peer},
            device_id_type=MESH,
        )

    def arrived(slot, count, first):
        view = table.at[pl.ds(0, count), pl.ds(first, RING_Y - first)]
        pltpu.make_async_remote_copy(
            src_ref=view,
            dst_ref=view,
            send_sem=y_send.at[0],
            recv_sem=arrival(slot),
            device_id={"kv": up},
            device_id_type=MESH,
        ).wait_recv()

    def pass_on(slot):
        stage[...] = kvbuf[slot]
        for d in (2, 1, 3):
            outbox[slot, d] = stage[want_smem[d, 0, d * ring_z + slot]]
        table[slot, 0] = stage[want_smem[0, 0, slot]]
        for d in (2, 1, 3):
            chosen_copy(d, slot, side[d], 0).start()

    def pass_beyond(dz, held, slot):
        stage[...] = kvbuf[held]
        for d in (2, 1, 3, 0):
            row_there = (RING_Y if dz == 1 else 2 * RING_Y) + d
            outbox[slot, d] = stage[want_smem[row_there, 0, d * ring_z + slot]]
        for d in (2, 1, 3, 0):
            chosen_copy(d, slot, beyond[dz][d], 1 if dz == 1 else 2).start()

    near_keys = RING_Y * block_rows

    def attend_slots(tile, slots):
        if tile is None or tile[0] == 0:
            lane_row = lax.broadcasted_iota(jnp.int32, (near_keys, 128), 1)
            back = lax.broadcasted_iota(jnp.int32, (near_keys, 128), 0) // block_rows * ring_z
            for i, slot in enumerate(slots):
                both = table[slot].reshape(near_keys, 2 * HEAD_WIDTH)
                here = slice(i * near_keys, (i + 1) * near_keys)
                keys_in[here, 0:HEAD_WIDTH] = both[:, 0:HEAD_WIDTH]
                keys_in[here, HEAD_WIDTH:] = jnp.where(
                    lane_row == back + slot, 1.0, 0.0
                ).astype(bf16)
                values_in[:, here] = both[:, HEAD_WIDTH:].T
        attend(tile, len(slots) * near_keys, False)

    def due_from_above(t, c):
        behind = (t - 1) * chunks + c - (LAG[0] * (ring_z - 1 - z)) // LAG[1]
        m = jnp.maximum(behind, 0)
        crossed = z > last_down
        hops = jnp.where(crossed, m // chunks + ring_z - z, t)
        chunk = jnp.where(crossed, m % chunks, c)
        due = jnp.where(crossed, (behind >= 0) & (hops <= last_down), from_above(t))
        return due, hops, chunk

    def step(t, fill):
        for c in range(chunks):

            if t is not last_up:

                @pl.when(from_below(t))
                def _():
                    ring_copy(True, t, t, c).wait_recv()

            elif c == chunks - 1:

                @pl.when(from_below(t))
                def _():
                    whole_slot(True, t, t).wait_recv()

            @pl.when(to_above(t))
            def _():
                ring_copy(True, t, t + 1, c).start()

            due, hops, chunk = due_from_above(t, c)
            back = ring_z - hops

            @pl.when(due & (hops < last_down))
            def _():
                ring_copy(False, back, back, chunk).wait_recv()

            @pl.when(due & (hops == last_down) & (chunk == chunks - 1))
            def _():
                whole_slot(False, ring_z - last_down, last_down).wait_recv()

            @pl.when(due & (hops < last_down))
            def _():
                ring_copy(False, back, back - 1, chunk).start()

            @pl.when(due & (chunk == chunks - 1) & (hops == last_down) & chosen_down)
            def _():
                pass_beyond(ring_z - 1, ring_z - last_down, half)

            @pl.when(due & (chunk == chunks - 1) & (z >= back))
            def _():
                pass_on(back)

            if c < chunks - 1:
                fill(c)

        if t is last_up:

            @pl.when(chosen_up)
            def _():
                pass_beyond(1, last_up, last_up + 1)

        if t is not last_down:

            @pl.when(z >= t)
            def _():
                pass_on(t)

        fill(chunks - 1)

    def near_slots(t):
        @pl.when((z >= t) & (z < ring_z - t))
        def _():
            arrived(t, 1, 1)

        @pl.when(z >= ring_z - t)
        def _():
            arrived(t, 2, 1)

    near_scalars = pltpu.make_async_copy(want_all.at[row], want_smem.at[row], load_sem.at[3])
    far_rows = pl.ds(RING_Y, 2 * RING_Y)
    far_scalars = pltpu.make_async_copy(want_all.at[far_rows], want_smem.at[far_rows], load_sem.at[3])

    def fill_first(c):
        if c == 1:
            want_side.wait()
            want_up.start()
            want_down.start()
            near_scalars.start()
        if c == chunks - 2:
            near_scalars.wait()
            pass_on(0)

    def fill_second(c):
        if c == chunks - 1:
            want_up.wait()
            want_down.wait()
            far_scalars.start()
            arrived(0, 1, 1)
            attend_slots(None, [0])
            far_scalars.wait()

    def fill_near(t, c):
        if c == 1:
            near_slots(t)
        wide = 3 * COLUMN_TILE
        for tile in {1: [(0, wide)], 3: [(wide, columns - wide)]}.get(c, []):

            @pl.when(z >= t)
            def _():
                attend_slots(tile, [t, ring_z - t])

    share = pltpu.make_async_remote_copy(
        src_ref=attended,
        dst_ref=partner,
        send_sem=tp_send,
        recv_sem=tp_recv,
        device_id={"tp": 1 - core},
        device_id_type=MESH,
    )

    def finish():
        with jax.named_scope("normalise"):
            for tile in range(tiles):
                here = slice(tile * COLUMN_TILE, (tile + 1) * COLUMN_TILE)
                by_row[here, :] = (acc[:, here] / l_ref[:, here]).T.astype(bf16)
            for h in range(heads):
                attended[:, h * HEAD_WIDTH : (h + 1) * HEAD_WIDTH] = by_row[
                    h * rows : (h + 1) * rows, :
                ]
            load_wo.wait()
            share.start()
            width = heads * HEAD_WIDTH
            mine = pl.ds(pl.multiple_of(core * width, width), width)
            own_mixed[...] = jnp.dot(attended[...], wo[mine, :], preferred_element_type=f32)

        mass = m_ref[...] * LN_2 + jnp.log(l_ref[...])
        for h in range(heads):
            log_out[0, h : h + 1, :] = mass[:, h * rows : (h + 1) * rows]

    with jax.named_scope("own"):
        attend_own()
    with jax.named_scope("step_1"):
        step(1, fill_first)
    with jax.named_scope("step_2"):
        step(2, fill_second)

    @pl.loop(3, last_up)
    def _(t):
        with jax.named_scope("step_t"):
            step(t, functools.partial(fill_near, t - 2))

    @pl.when(z == 0)
    def _():
        finish()

    with jax.named_scope("step_6"):
        step(last_up, functools.partial(fill_near, last_up - 2))
    with jax.named_scope("step_7"):
        step(last_down, functools.partial(fill_near, last_down - 2))

    with jax.named_scope("last_but_one"):
        near_slots(last_up)

        @pl.when(z > last_up)
        def _():
            arrived(last_up + 1, 1, 0)

        @pl.when(z >= last_up)
        def _():
            attend_slots(None, [last_up, ring_z - last_up, last_up + 1])

    with jax.named_scope("last_wait"):

        @pl.when(z >= half)
        def _():
            arrived(half, 1, 0)

        @pl.when(z > half)
        def _():
            arrived(half + 1, 1, 1)

    with jax.named_scope("last"):

        @pl.when(z >= half)
        def _():
            attend_slots(None, [half, half + 1])

    @pl.when(z > 0)
    def _():
        finish()

    with jax.named_scope("sends"):
        ups = jnp.where(z < ring_z - 1, jnp.minimum(z + 1, last_up), 0)
        for n in range(1, last_up + 1):

            @pl.when(ups == n)
            def _():
                sent(kvbuf, plus_send.at[0], n)

        downs = jnp.where(
            z <= last_down,
            jnp.minimum(last_down + 1 - z, last_down),
            jnp.maximum(z - (ring_z - last_down), 0),
        )
        for n in range(1, last_down + 1):

            @pl.when(downs == n)
            def _():
                sent(kvbuf, minus_send.at[0], n)

        passes = jnp.minimum(z, last_up) + jnp.maximum(z - (ring_z - last_down - 1), 0) + 1
        for n in range(1, last_up + last_down + 2):

            @pl.when(passes == n)
            def _():
                sent(outbox.at[:, pl.ds(1, RING_Y - 1)], y_send.at[0], n)

        @pl.when(chosen_up)
        def _():
            sent(outbox, y_send.at[1], 1)

        @pl.when(chosen_down)
        def _():
            sent(outbox, y_send.at[2], 1)

    share.wait()


def mix_kernel(partner, wo, own_mixed, log_in, mixed_hbm, log_hbm, mixed, log_vmem, sem):
    width = partner.shape[1]
    other = 1 - lax.axis_index("tp")
    theirs = pl.ds(pl.multiple_of(other * width, width), width)
    log_vmem[...] = log_in[...]
    copies = [pltpu.make_async_copy(log_vmem, log_hbm, sem.at[0])]
    copies[0].start()
    step = wo.shape[1] // MIX_PARTS
    for i in range(MIX_PARTS):
        here = slice(i * step, (i + 1) * step)
        mixed[0, :, here] = (
            own_mixed[:, here]
            + jnp.dot(partner[...], wo[theirs, here], preferred_element_type=jnp.float32)
        ).astype(jnp.bfloat16)
        copy = pltpu.make_async_copy(
            mixed.at[:, :, pl.ds(i * step, step)], mixed_hbm.at[:, :, pl.ds(i * step, step)], sem.at[i + 1]
        )
        copy.start()
        copies.append(copy)
    for copy in copies:
        copy.wait()


def body(tokens, w_query, key_weight, value_weight, w_out, chosen):
    row_count, depth = tokens.shape[1], tokens.shape[2]
    blocks_here, slots = chosen.shape[1:]
    block_rows = row_count // blocks_here
    ring_z = lax.axis_size("kv") // RING_Y
    q_width = w_query.shape[1]
    heads = q_width // HEAD_WIDTH
    kv_width = key_weight.shape[1] + value_weight.shape[1]
    chunks = blocks_here // BLOCKS_PER_CHUNK
    dma = pltpu.SemaphoreType.DMA
    vmem = pltpu.VMEM
    hbm = lambda x: pltpu.with_memory_space_constraint(x, pltpu.HBM)
    partner, log_part, wo, own_mixed = pl.pallas_call(
        functools.partial(exchange_kernel, ring_z, blocks_here, block_rows),
        out_shape=(
            vmem((row_count, q_width), jnp.bfloat16),
            vmem((1, heads, row_count), jnp.float32),
            vmem(w_out.shape, jnp.bfloat16),
            vmem((row_count, w_out.shape[1]), jnp.float32),
        ),
        in_specs=[pl.BlockSpec(memory_space=pl.ANY)] * 6,
        out_specs=(pl.BlockSpec(memory_space=vmem),) * 4,
        scratch_shapes=[
            vmem((row_count, depth), jnp.bfloat16),
            vmem((depth, kv_width), jnp.bfloat16),
            vmem((depth, q_width), jnp.bfloat16),
            vmem((row_count, kv_width), jnp.float32),
            vmem((blocks_here, 1, slots), jnp.int32),
            vmem((ring_z, blocks_here, block_rows, kv_width), jnp.bfloat16),
            vmem((blocks_here, block_rows, kv_width), jnp.bfloat16),
            vmem((ring_z, RING_Y, block_rows, kv_width), jnp.bfloat16),
            vmem((ring_z, RING_Y, block_rows, kv_width), jnp.bfloat16),
            vmem((heads * row_count, 2 * HEAD_WIDTH), jnp.bfloat16),
            vmem((1, heads * row_count), jnp.float32),
            vmem((1, heads * row_count), jnp.float32),
            vmem((HEAD_WIDTH, heads * row_count), jnp.float32),
            vmem((max(row_count, 3 * RING_Y * block_rows), 2 * HEAD_WIDTH), jnp.bfloat16),
            vmem((HEAD_WIDTH, max(row_count, 3 * RING_Y * block_rows)), jnp.bfloat16),
            vmem((heads * row_count, HEAD_WIDTH), jnp.bfloat16),
            vmem((row_count, q_width), jnp.bfloat16),
            vmem((3 * RING_Y, 1, 128), jnp.int32),
            pltpu.SMEM((3 * RING_Y, 1, 128), jnp.int32),
            dma((4,)),
            dma((DEPTH_PARTS, 2)),
            dma((1,)),
            dma(((ring_z // 2 - 3) * chunks + 1,)),
            dma((1,)),
            dma(((ring_z // 2 - 2) * chunks + 1,)),
            dma((3,)),
            dma((ring_z // 2 + 2,)),
            dma((3,)),
            dma((3,)),
            dma,
            dma,
        ],
        compiler_params=pltpu.CompilerParams(
            collective_id=0, has_side_effects=True, vmem_limit_bytes=40 * 1024 * 1024
        ),
    )(*map(hbm, (tokens, w_query, key_weight, value_weight, w_out, chosen.reshape(blocks_here, 1, slots))))
    return pl.pallas_call(
        mix_kernel,
        out_shape=(
            jax.ShapeDtypeStruct((1, row_count, w_out.shape[1]), jnp.bfloat16),
            jax.ShapeDtypeStruct((1, heads, row_count), jnp.float32),
        ),
        in_specs=[pl.BlockSpec(memory_space=vmem)] * 4,
        out_specs=(pl.BlockSpec(memory_space=pl.ANY),) * 2,
        scratch_shapes=[
            vmem((1, row_count, w_out.shape[1]), jnp.bfloat16),
            vmem((1, heads, row_count), jnp.float32),
            dma((MIX_PARTS + 1,)),
        ],
        compiler_params=pltpu.CompilerParams(vmem_limit_bytes=12 * 1024 * 1024),
    )(partner, wo, own_mixed, log_part)


def solution(mesh):
    in_specs = (
        P("dp", "kv", None),
        P(None, "tp"),
        P(None, "tp"),
        P(None, "tp"),
        P(None, "tp"),
        P("dp", "kv", None),
    )
    out_specs = (P("dp", "kv", "tp"), P("dp", "tp", "kv"))
    return jax.shard_map(body, mesh=mesh, in_specs=in_specs, out_specs=out_specs, check_vma=False)
```
